256 devices in a mesh: grp: 2 (over y), sp: 32 (over z, core), tp: 4 (over x).
Axes of the slice: x: 4, y: 2, z: 16, core: 2. Of those that a mesh axis runs over, the one named last changes fastest.
The devices are a block of a 4x16x16 slice.
Arguments:
- residual: bfloat16 [49152, 2048], P(('grp', 'sp', 'tp')), parts along dimension 0, may hold values from -6 to 6
- value_projected: bfloat16 [49152, 4096], P(('grp', 'sp'), 'tp'), parts along dimension 0, may hold values from -6 to 6
- gate_projected: bfloat16 [49152, 4096], P(('grp', 'sp'), 'tp'), parts along dimension 0, may hold values from -6 to 6
- wide_key_rows: bfloat16 [49152, 1024], P(('grp', 'sp'), 'tp'), parts along dimension 0, may hold values from -6 to 6
- wide_query_rows: bfloat16 [49152, 1024], P(('grp', 'sp'), 'tp'), parts along dimension 0, may hold values from -6 to 6
- narrow_key_rows: bfloat16 [49152, 512], P(('grp', 'sp'), 'tp'), parts along dimension 0, may hold values from -6 to 6
- narrow_query_rows: bfloat16 [49152, 512], P(('grp', 'sp'), 'tp'), parts along dimension 0, may hold values from -6 to 6
- step_before_softplus: float32 [49152, 64], P(('grp', 'sp'), 'tp'), parts along dimension 0, may hold values from -5 to 5
- extra_log_decay: float32 [49152, 64], P(('grp', 'sp'), 'tp'), parts along dimension 0, may hold values from -0.7 to 0
- log_decay_rate: float32 [64], P('tp'), may hold values from -12.3 to -2.99
- value_kernel: bfloat16 [4, 4096], P(None, 'tp'), may hold values from -3 to 3
- wide_key_kernel: bfloat16 [4, 1024], P(None, 'tp'), may hold values from -3 to 3
- wide_query_kernel: bfloat16 [4, 1024], P(None, 'tp'), may hold values from -3 to 3
- narrow_key_kernel: bfloat16 [4, 512], P(None, 'tp'), may hold values from -3 to 3
- narrow_query_kernel: bfloat16 [4, 512], P(None, 'tp'), may hold values from -3 to 3
- head_norm_gain: bfloat16 [4096], P('tp'), may hold values from 0.099609375 to 1.8984375
- output_matrix: bfloat16 [4096, 2048], P('tp'), may hold values from -0.09375 to 0.09375
- feedforward_norm_gain: bfloat16 [2048], replicated, may hold values from 0.099609375 to 1.8984375
- gate_matrix: bfloat16 [2048, 3072], P('sp', 'tp'), may hold values from -0.125 to 0.125
- up_matrix: bfloat16 [2048, 3072], P('sp', 'tp'), may hold values from -0.125 to 0.125
- down_matrix: bfloat16 [2048, 3072], P('sp', 'tp'), may hold values from -0.3125 to 0.3125
Outputs:
- mixed: bfloat16 [49152, 2048], P(('grp', 'sp', 'tp')), parts along dimension 0
The draws below stay inside these ranges and needn't reach their ends.
There are 2 independent parts, one for each index of `grp`. The reference program is written for one: setup_inputs(seed, part) draws one part's arguments, and reference() takes and returns one part's arrays. A program takes and returns all parts, laid end to end along the dimension named above; an argument that names none is the same for every part. Nothing has to cross between parts.
All inputs are finite; a program needn't handle non-finite values.
Results may differ from the reference program's by a relative error of at most 0.015.
Values may be sent and summed in bfloat16 or wider, within the bound.
A program may use at most 128 MiB of HBM per device.

```python
import math
import jax
import jax.numpy as jnp
from jax import lax

D = 2048
HEADS = 64
HEAD_DIM = 64
GROUPS = 16
STATE_WIDE = 128
STATE_NARROW = 64
FF = 3072
CONV_W = 4
BLK = 64
TOK_DEV = 768
INNER = 4096
TOKENS = 24576
N_TP = 4


def draw_step_before_softplus(key, part):
    noise_key, shift_key = jax.random.split(jax.random.fold_in(key, 11))
    count = TOKENS // TOK_DEV
    shifts = jax.random.uniform(shift_key, (count, 1, HEADS), jnp.float32, -1.0, 1.0)
    noise = jnp.clip(jax.random.normal(noise_key, (count, TOK_DEV, HEADS), jnp.float32), -4.0, 4.0)
    return (noise + shifts).reshape(TOKENS, HEADS)


def draw_extra_log_decay(key, part):
    place_key, loss_key = jax.random.split(jax.random.fold_in(key, 23))
    places = jax.random.randint(place_key, (2, HEADS), 0, TOKENS)
    losses = jax.random.uniform(loss_key, (2, HEADS), jnp.float32, 0.2, 0.5)
    positions = jnp.arange(TOKENS, dtype=jnp.int32)[:, None]
    total = jnp.zeros((TOKENS, HEADS), jnp.float32)
    for number in range(2):
        total = total + jnp.where(positions == places[number][None, :], jnp.log(1.0 - losses[number])[None, :], 0.0)
    return total


def draw_log_decay_rate(key, part):
    order_key, slow_key, fast_key = jax.random.split(jax.random.fold_in(key, 37), 3)
    order = jax.random.permutation(order_key, HEADS)
    fast_count = HEADS // 2
    slow = math.log(5e-06) + jax.random.uniform(slow_key, (HEADS,), jnp.float32) * math.log(4.0)
    fast = math.log(0.03) + jax.random.uniform(fast_key, (HEADS,), jnp.float32) * math.log(0.05 / 0.03)
    return jnp.where(order < fast_count, fast, slow)


def steps_of(key, extent, shards, least, top_value):
    level = 1.0
    for position, blocks in shards:
        draws = jax.random.uniform(jax.random.fold_in(jax.random.fold_in(key, 6), position), (blocks,), jnp.float32, least / len(shards), top_value / len(shards))
        level = level * jnp.repeat(jnp.exp(draws), extent[position] // blocks).reshape((-1,) + (1,) * (len(extent) - 1 - position))
    return level


def normal_values(own_key, dims, scale, bound, shards=(), kind=jnp.bfloat16):
    result = jax.random.normal(own_key, dims, jnp.float32) * scale
    if len(shards) > 0:
        result = steps_of(own_key, dims, shards, -0.22, 0.18) * result
    return jnp.clip(result, min=-bound, max=bound).astype(kind)


def setup_inputs(seed: int = 0, part: int = 0) -> dict:
    seeds = jax.random.split(jax.random.key(seed), 22)
    part_keys = jax.random.split(jax.random.fold_in(seeds[21], part), 22)
    return {
        "residual": normal_values(part_keys[0], (TOKENS, D), 1.0, 6.0, ((0, 128),)),
        "value_projected": normal_values(part_keys[1], (TOKENS, INNER), 1.0, 6.0, ((0, 32), (1, 4))),
        "gate_projected": normal_values(part_keys[2], (TOKENS, INNER), 1.0, 6.0, ((0, 32), (1, 4))),
        "wide_key_rows": normal_values(part_keys[3], (TOKENS, GROUPS * STATE_WIDE // 2), 1.0, 6.0, ((0, 32), (1, 4))),
        "wide_query_rows": normal_values(part_keys[4], (TOKENS, GROUPS * STATE_WIDE // 2), 1.0, 6.0, ((0, 32), (1, 4))),
        "narrow_key_rows": normal_values(part_keys[5], (TOKENS, GROUPS * STATE_NARROW // 2), 1.0, 6.0, ((0, 32), (1, 4))),
        "narrow_query_rows": normal_values(part_keys[6], (TOKENS, GROUPS * STATE_NARROW // 2), 1.0, 6.0, ((0, 32), (1, 4))),
        "step_before_softplus": draw_step_before_softplus(jax.random.fold_in(jax.random.fold_in(seeds[21], part), 71), part),
        "extra_log_decay": draw_extra_log_decay(jax.random.fold_in(jax.random.fold_in(seeds[21], part), 71), part),
        "log_decay_rate": draw_log_decay_rate(jax.random.fold_in(seeds[21], 71), part),
        "value_kernel": normal_values(seeds[10], (CONV_W, INNER), CONV_W ** -0.5, 3.0, ((1, 4),)),
        "wide_key_kernel": normal_values(seeds[11], (CONV_W, GROUPS * STATE_WIDE // 2), CONV_W ** -0.5, 3.0, ((1, 4),)),
        "wide_query_kernel": normal_values(seeds[12], (CONV_W, GROUPS * STATE_WIDE // 2), CONV_W ** -0.5, 3.0, ((1, 4),)),
        "narrow_key_kernel": normal_values(seeds[13], (CONV_W, GROUPS * STATE_NARROW // 2), CONV_W ** -0.5, 3.0, ((1, 4),)),
        "narrow_query_kernel": normal_values(seeds[14], (CONV_W, GROUPS * STATE_NARROW // 2), CONV_W ** -0.5, 3.0, ((1, 4),)),
        "head_norm_gain": jnp.clip(1.0 + 0.18 * jax.random.normal(seeds[15], (INNER,), jnp.float32), 0.099609375, 1.8984375).astype(jnp.bfloat16),
        "output_matrix": normal_values(seeds[16], (INNER, D), INNER ** -0.5, 0.09375, ((0, 4),)),
        "feedforward_norm_gain": jnp.clip(1.0 + 0.18 * jax.random.normal(seeds[17], (D,), jnp.float32), 0.099609375, 1.8984375).astype(jnp.bfloat16),
        "gate_matrix": normal_values(seeds[18], (D, FF), D ** -0.5, 0.125, ((0, 32), (1, 4))),
        "up_matrix": normal_values(seeds[19], (D, FF), D ** -0.5, 0.125, ((0, 32), (1, 4))),
        "down_matrix": normal_values(seeds[20], (D, FF), (FF // 9) ** -0.5, 0.3125, ((0, 32), (1, 4))),
    }


def to_half(value):
    return lax.optimization_barrier(value.astype(jnp.bfloat16)).astype(jnp.float32)

def short_conv(inputs, kernel):
    width = kernel.shape[0]
    length = inputs.shape[0]
    padded = jnp.pad(inputs.astype(jnp.float32), ((width - 1, 0), (0, 0)))
    total = jnp.zeros(inputs.shape, jnp.float32)
    for offset in range(width):
        total = total + padded[offset:offset + length] * kernel[offset].astype(jnp.float32)
    return jax.nn.silu(total).astype(jnp.bfloat16)

def family_mix(values, step_sizes, decay_factor, keys, queries):
    length, groups, per_group, width = values.shape
    states = keys.shape[2]
    count = length // BLK
    lower = jnp.tril(jnp.ones((BLK, BLK), dtype=bool))
    highest = lax.Precision.HIGHEST

    def advance(carried, block):
        block_values, block_steps, block_decay, block_keys, block_queries = block
        values32 = block_values.astype(jnp.float32)
        keys32 = block_keys.astype(jnp.float32)
        queries32 = block_queries.astype(jnp.float32)
        running = jnp.cumsum(block_decay, axis=0)
        scores = jnp.einsum('lgn,sgn->lsg', queries32, keys32, precision=highest)
        spread = jnp.where(lower[:, :, None, None], running[:, None] - running[None, :], -jnp.inf)
        weights = to_half(scores[..., None] * jnp.exp(spread) * block_steps[None])
        inside = jnp.einsum('lsgr,sgrp->lgrp', weights, values32, precision=highest)
        outside = jnp.exp(running)[..., None] * jnp.einsum('lgn,grpn->lgrp', queries32, to_half(carried), precision=highest)
        fade = block_steps * jnp.exp(running[-1][None] - running)
        scaled = to_half(values32 * fade[..., None])
        block_state = jnp.einsum('lgrp,lgn->grpn', scaled, keys32, precision=highest)
        carried = jnp.exp(running[-1])[..., None, None] * carried + block_state
        return (carried, inside + outside)
    blocks = (values.reshape(count, BLK, groups, per_group, width), step_sizes.reshape(count, BLK, groups, per_group), decay_factor.reshape(count, BLK, groups, per_group), keys.reshape(count, BLK, groups, states), queries.reshape(count, BLK, groups, states))
    initial = jnp.zeros((groups, per_group, width, states), jnp.float32)
    ending, outputs = lax.scan(advance, initial, blocks)
    return outputs.reshape(length, groups, per_group, width)

def reference(residual, value_projected, gate_projected, wide_key_rows, wide_query_rows, narrow_key_rows, narrow_query_rows, step_before_softplus, extra_log_decay, log_decay_rate, value_kernel, wide_key_kernel, wide_query_kernel, narrow_key_kernel, narrow_query_kernel, head_norm_gain, output_matrix, feedforward_norm_gain, gate_matrix, up_matrix, down_matrix):
    length = value_projected.shape[0]
    per_group = HEADS // GROUPS
    half = GROUPS // 2
    values = short_conv(value_projected, value_kernel).reshape(length, half, 2, per_group, HEAD_DIM)
    keys_w = short_conv(wide_key_rows, wide_key_kernel).reshape(length, half, STATE_WIDE)
    queries_w = short_conv(wide_query_rows, wide_query_kernel).reshape(length, half, STATE_WIDE)
    keys_n = short_conv(narrow_key_rows, narrow_key_kernel).reshape(length, half, STATE_NARROW)
    queries_n = short_conv(narrow_query_rows, narrow_query_kernel).reshape(length, half, STATE_NARROW)
    step_sizes = jax.nn.softplus(step_before_softplus)
    decay_factor = -jnp.exp(log_decay_rate)[None, :] * step_sizes + extra_log_decay
    step_sizes = step_sizes.reshape(length, half, 2, per_group)
    decay_factor = decay_factor.reshape(length, half, 2, per_group)
    wide = family_mix(values[:, :, 0], step_sizes[:, :, 0], decay_factor[:, :, 0], keys_w, queries_w)
    narrow = family_mix(values[:, :, 1], step_sizes[:, :, 1], decay_factor[:, :, 1], keys_n, queries_n)
    heads_out = jnp.stack([wide, narrow], axis=2).reshape(length, HEADS, HEAD_DIM)
    gated = heads_out * jax.nn.silu(gate_projected.astype(jnp.float32)).reshape(length, HEADS, HEAD_DIM)
    gated = gated * lax.rsqrt(lax.optimization_barrier(jnp.mean(gated * gated, axis=-1, keepdims=True)) + 1e-06)
    normed = (gated.reshape(length, INNER) * head_norm_gain.astype(jnp.float32)).astype(jnp.bfloat16)
    share = INNER // N_TP
    projected = jnp.zeros((length, D), jnp.float32)
    for index in range(N_TP):
        partial_value = jnp.dot(normed[:, index * share:(index + 1) * share], output_matrix[index * share:(index + 1) * share], preferred_element_type=jnp.float32)
        projected = projected + to_half(partial_value)
    after_mixer = (residual.astype(jnp.float32) + projected).astype(jnp.bfloat16)
    rows = after_mixer.astype(jnp.float32)
    x_norm = (rows * lax.rsqrt(lax.optimization_barrier(jnp.mean(rows * rows, axis=-1, keepdims=True)) + 1e-06) * feedforward_norm_gain.astype(jnp.float32)).astype(jnp.bfloat16)
    gate_values = jnp.dot(x_norm, gate_matrix, preferred_element_type=jnp.float32)
    up_values = jnp.dot(x_norm, up_matrix, preferred_element_type=jnp.float32)
    hidden = (jax.nn.silu(gate_values) * up_values).astype(jnp.bfloat16)
    portion = FF // N_TP
    channel = jnp.zeros((length, D), jnp.float32)
    for index in range(N_TP):
        partial_value = lax.dot_general(hidden[:, index * portion:(index + 1) * portion], down_matrix[:, index * portion:(index + 1) * portion], (((1,), (1,)), ((), ())), preferred_element_type=jnp.float32)
        channel = channel + to_half(partial_value)
    return (after_mixer.astype(jnp.float32) + 0.5 * channel).astype(jnp.bfloat16)
```

```python
import functools
import jax
import jax.numpy as jnp
from jax import lax
from jax.experimental import pallas as pl
from jax.experimental.pallas import tpu as pltpu
from jax.sharding import PartitionSpec as P

F32 = jnp.float32
BF16 = jnp.bfloat16
MESH = pl.DeviceIdType.MESH
CH = 128
PAD = 16
GROUP_Q = (0, 256, 128, 384)
GROUP_K = (0, 256, 128, 256)
ROW_GROUP = ((0, 128, 0), (128, 256, 2), (256, 320, 1), (320, 384, 3))
HIGH = lax.Precision.HIGHEST


def pair_lanes(columns, head):
    rows = columns.shape[0]
    lane = lax.broadcasted_iota(jnp.int32, (rows, 128), 1)
    return jnp.where(
        lane < 64,
        jnp.broadcast_to(columns[:, head : head + 1], (rows, 128)),
        jnp.broadcast_to(columns[:, head + 1 : head + 2], (rows, 128)),
    )


def quad_lanes(columns, group):
    return jnp.concatenate(
        [pair_lanes(columns, 4 * group), pair_lanes(columns, 4 * group + 2)], axis=1
    )


def silu(x):
    return x / (1.0 + jnp.exp(-x))


def matmul(a, b, dims=((1,), (0,)), precision=None):
    return lax.dot_general(a, b, (dims, ((), ())), preferred_element_type=F32, precision=precision)


def group_of_row(row):
    for low, high, group in ROW_GROUP:
        if low <= row < high:
            return group


def mixer_kernel(
    peers,
    value_ref,
    wk_ref,
    wq_ref,
    nk_ref,
    nq_ref,
    gate_ref,
    step_ref,
    extra_ref,
    rate_ref,
    vker_ref,
    wkker_ref,
    wqker_ref,
    nkker_ref,
    nqker_ref,
    gain_ref,
    normed_ref,
    xpad,
    ubuf,
    kbuf,
    qbuf,
    gbuf,
    rcol,
    qrow,
    total,
    ebuf,
    hbuf,
    ybuf,
    out_msg,
    in_msg,
    out_ret,
    in_ret,
    hent,
    local_sem,
    rim_send,
    rim_recv,
    send_a,
    recv_a,
    send_b,
    recv_b,
):
    length = value_ref.shape[0]
    count = length // CH
    me = lax.axis_index("sp")
    inputs = (value_ref, wk_ref, wq_ref, nk_ref, nq_ref)
    spans = []
    at = 0
    for ref in inputs:
        spans.append((at, at + ref.shape[1]))
        at += ref.shape[1]
    loads = [
        pltpu.make_async_copy(
            ref, xpad.at[pl.ds(PAD, length), pl.ds(low, high - low)], local_sem.at[n]
        )
        for n, (ref, (low, high)) in enumerate(zip(inputs, spans))
    ]
    loads.append(pltpu.make_async_copy(gate_ref, gbuf, local_sem.at[len(inputs)]))
    for load in loads:
        load.start()
    rims = []
    if peers > 1:
        barrier = pltpu.get_barrier_semaphore()
        for offset in range(1, peers):
            pl.semaphore_signal(
                barrier,
                inc=1,
                device_id={"sp": lax.rem(me + offset, peers)},
                device_id_type=MESH,
            )
        pl.semaphore_wait(barrier, peers - 1)
        for n, (ref, (low, high)) in enumerate(zip(inputs, spans)):
            rims.append(
                pltpu.make_async_remote_copy(
                    src_ref=ref.at[pl.ds(length - PAD, PAD)],
                    dst_ref=xpad.at[pl.ds(0, PAD), pl.ds(low, high - low)],
                    send_sem=rim_send.at[n],
                    recv_sem=rim_recv.at[n],
                    device_id={"sp": lax.rem(me + 1, peers)},
                    device_id_type=MESH,
                )
            )
        for rim in rims:
            rim.start()
    for load in loads[:-1]:
        load.wait()

    row_id = lax.broadcasted_iota(jnp.int32, (CH, CH), 0)
    col_id = lax.broadcasted_iota(jnp.int32, (CH, CH), 1)
    lower = row_id >= col_id
    tril = lower.astype(F32)
    triu = (row_id <= col_id).astype(F32)
    eye = (row_id == col_id).astype(F32)
    left = lax.broadcasted_iota(jnp.int32, (CH, 128), 1) < 64
    kernels = (vker_ref, wkker_ref, wqker_ref, nkker_ref, nqker_ref)

    def conv_tile(base, which, tile):
        low = spans[which][0] + 128 * tile
        columns = pl.ds(low, 128)
        before = xpad[pl.ds(base, PAD), columns].astype(F32)[PAD - 8 :]
        here = xpad[pl.ds(base + PAD, CH), columns].astype(F32)
        rows = jnp.concatenate([before, here], axis=0)
        taps = kernels[which][:, 128 * tile : 128 * tile + 128].astype(F32)
        acc = here * taps[3:4]
        for tap in range(3):
            acc = acc + pltpu.roll(rows, 3 - tap, 0)[8:] * taps[tap : tap + 1]
        return silu(acc)

    def first_pass(i, carry):
        c = lax.rem(i + 1, count)
        base = pl.multiple_of(c * CH, CH)

        @pl.when(i == count - 1)
        def _():
            for rim in rims:
                rim.wait()

            @pl.when(me == 0)
            def _():
                xpad[0:PAD, :] = jnp.zeros((PAD, xpad.shape[1]), BF16)

        here = pl.ds(base, CH)
        dt = step_ref[here, :]
        dt = jnp.maximum(dt, 0.0) + jnp.log(1.0 + jnp.exp(-jnp.abs(dt)))
        a = -jnp.exp(rate_ref[...]) * dt + extra_ref[here, :]
        r = matmul(tril, a, precision=HIGH)
        r_row = matmul(a, triu, ((0,), (0,)), HIGH)
        dt_row = matmul(dt, eye, ((0,), (0,)), HIGH)
        rcol[here, :] = r
        qrow[c] = r_row - jnp.log(dt_row)
        end = r[CH - 1 : CH, :]
        total[c] = end
        fade = dt * jnp.exp(end - r)
        for tile in range(2):
            kbuf[here, 128 * tile : 128 * tile + 128] = conv_tile(base, 1, tile).astype(BF16)
            qbuf[here, 128 * tile : 128 * tile + 128] = conv_tile(base, 2, tile).astype(BF16)
        kbuf[here, 256:384] = conv_tile(base, 3, 0).astype(BF16)
        narrow_q = conv_tile(base, 4, 0)
        qbuf[here, 256:384] = jnp.where(left, narrow_q, 0.0).astype(BF16)
        qbuf[here, 384:512] = jnp.where(left, 0.0, narrow_q).astype(BF16)
        for group in range(4):
            parts = []
            for half in range(2):
                pair = 2 * group + half
                u = conv_tile(base, 0, pair).astype(BF16)
                ubuf[here, 128 * pair : 128 * pair + 128] = u
                parts.append((u.astype(F32) * pair_lanes(fade, 2 * pair)).astype(BF16))
            v = jnp.concatenate(parts, axis=1)
            k = kbuf[here, GROUP_K[group] : GROUP_K[group] + 128]
            e = matmul(k, v, ((0,), (0,)))
            if group == 0:
                ebuf[c, 0:128, :] = e
            elif group == 2:
                ebuf[c, 128:256, :] = e
            elif group == 1:
                ebuf[c, 256:320, :] = e[0:64]
            else:
                ebuf[c, 320:384, :] = e[64:128]
        return carry

    lax.fori_loop(0, count, first_pass, 0)

    offsets = [jnp.zeros((1, 16), F32)]
    for c in range(count):
        offsets.append(offsets[-1] + total[c])
    whole = offsets[-1]
    for low, high, group in ROW_GROUP:
        state = jnp.zeros((high - low, 256), F32)
        for c in range(count):
            hbuf[c, low:high, :] = state.astype(BF16)
            state = state * jnp.exp(quad_lanes(total[c], group)) + ebuf[c, low:high, :]
        hent[low:high, :] = state

    if peers > 1:
        per = 384 // (peers // 2)
        wide_log = [quad_lanes(whole, group) for group in range(4)]
        sub = lax.broadcasted_iota(jnp.int32, (8, 128), 0)
        for slot in range(peers):
            z, core = slot // 2, slot % 2
            lanes = slice(128 * core, 128 * core + 128)
            logs = jnp.zeros((8, 128), F32)
            for tile in range(per // 8):
                line = wide_log[group_of_row(per * z + 8 * tile)][:, lanes]
                logs = jnp.where(sub == tile, jnp.broadcast_to(line, (8, 128)), logs)
            body = hent[per * z : per * z + per, lanes]
            out_msg[slot] = jnp.concatenate([body, logs], axis=0).astype(BF16)

        def exchange(source, target, send, recv):
            order = sorted(range(1, peers), key=lambda o: -min(o, peers - o))
            copies = []
            for offset in order:
                to = lax.rem(me + offset, peers)
                copies.append(
                    pltpu.make_async_remote_copy(
                        src_ref=source.at[to],
                        dst_ref=target.at[me],
                        send_sem=send.at[offset],
                        recv_sem=recv.at[offset],
                        device_id={"sp": to},
                        device_id_type=MESH,
                    )
                )
            return copies

        phase_a = exchange(out_msg, in_msg, send_a, recv_a)
        for copy in phase_a:
            copy.start()
        in_msg[me] = out_msg[me]

    for c in range(count):
        here = slice(c * CH, c * CH + CH)
        r = rcol[here, :]
        fade_out = jnp.exp(r)
        for group in range(4):
            q = qbuf[here, GROUP_Q[group] : GROUP_Q[group] + 128]
            k = kbuf[here, GROUP_K[group] : GROUP_K[group] + 128]
            score = matmul(q, k, ((1,), (1,)))
            row = 0 if group == 0 else 128 if group == 2 else 256
            outer = matmul(q, hbuf[c, row : row + 128, :])
            for half in range(2):
                pair = 2 * group + half
                weights = []
                for head in (2 * pair, 2 * pair + 1):
                    gap = jnp.broadcast_to(r[:, head : head + 1], (CH, CH)) - qrow[c, head : head + 1, :]
                    w = score * jnp.exp(jnp.where(lower, gap, -jnp.inf))
                    weights.append(w.astype(BF16))
                u = ubuf[here, 128 * pair : 128 * pair + 128].astype(F32)
                both = jnp.concatenate(
                    [jnp.where(left, u, 0.0).astype(BF16), jnp.where(left, 0.0, u).astype(BF16)],
                    axis=0,
                )
                inner = matmul(jnp.concatenate(weights, axis=1), both)
                ybuf[here, 128 * pair : 128 * pair + 128] = (
                    inner + outer[:, 128 * half : 128 * half + 128] * pair_lanes(fade_out, 2 * pair)
                )

    if peers > 1:
        for copy in phase_a:
            copy.wait()
        tiles = per // 8
        state = [jnp.zeros((8, 128), F32) for _ in range(tiles)]
        for source in range(peers):
            out_ret[source] = jnp.concatenate(
                state + [jnp.zeros((8, 128), F32)], axis=0
            ).astype(BF16)
            message = in_msg[source].astype(F32)
            for tile in range(tiles):
                decay = jnp.exp(message[per + tile : per + tile + 1, :])
                state[tile] = state[tile] * decay + message[8 * tile : 8 * tile + 8, :]
        phase_b = exchange(out_ret, in_ret, send_b, recv_b)
        for copy in phase_b:
            copy.start()
        in_ret[me] = out_ret[me]

    loads[-1].wait()
    if peers > 1:
        for copy in phase_b:
            copy.wait()
        for slot in range(peers):
            z, core = slot // 2, slot % 2
            hent[per * z : per * z + per, 128 * core : 128 * core + 128] = in_ret[slot].astype(
                F32
            )[:per]
    ones = (
        (row_id < 64) == (col_id < 64)
    ).astype(BF16)

    for c in range(count):
        here = slice(c * CH, c * CH + CH)
        reach = jnp.exp(rcol[here, :] + offsets[c])
        for group in range(4):
            if peers > 1:
                q = qbuf[here, GROUP_Q[group] : GROUP_Q[group] + 128]
                row = 0 if group == 0 else 128 if group == 2 else 256
                entered = matmul(q, hent[row : row + 128, :].astype(BF16))
            for half in range(2):
                pair = 2 * group + half
                lanes = slice(128 * pair, 128 * pair + 128)
                y = ybuf[here, lanes]
                if peers > 1:
                    y = y + entered[:, 128 * half : 128 * half + 128] * pair_lanes(reach, 2 * pair)
                gated = y * silu(gbuf[here, lanes].astype(F32))
                square = matmul((gated * gated).astype(BF16), ones)
                scale = lax.rsqrt(square * (1.0 / 64.0) + 1e-06)
                normed_ref[here, lanes] = (
                    gated * scale * gain_ref[:, lanes].astype(F32)
                ).astype(BF16)


def mixer(arrays, peers):
    length = arrays[0].shape[0]
    width = sum(a.shape[1] for a in arrays[:5])
    count = length // CH
    channels = arrays[0].shape[1]
    message = 384 // max(peers // 2, 1) + 8
    any_space = pl.BlockSpec(memory_space=pl.ANY)
    vmem = pl.BlockSpec(memory_space=pltpu.VMEM)
    dma = pltpu.SemaphoreType.DMA
    params = dict(vmem_limit_bytes=56 * 1024 * 1024)
    if peers > 1:
        params.update(collective_id=1, has_side_effects=True)
    return pl.pallas_call(
        functools.partial(mixer_kernel, peers),
        out_shape=jax.ShapeDtypeStruct((length, channels), BF16),
        in_specs=[any_space] * 6 + [vmem] * 9,
        out_specs=vmem,
        scratch_shapes=[
            pltpu.VMEM((PAD + length, width), BF16),
            pltpu.VMEM((length, channels), BF16),
            pltpu.VMEM((length, 384), BF16),
            pltpu.VMEM((length, 512), BF16),
            pltpu.VMEM((length, channels), BF16),
            pltpu.VMEM((length, 16), F32),
            pltpu.VMEM((count, 16, CH), F32),
            pltpu.VMEM((count, 1, 16), F32),
            pltpu.VMEM((count, 384, 256), F32),
            pltpu.VMEM((count, 384, 256), BF16),
            pltpu.VMEM((length, channels), F32),
            pltpu.VMEM((peers, message, 128), BF16),
            pltpu.VMEM((peers, message, 128), BF16),
            pltpu.VMEM((peers, message, 128), BF16),
            pltpu.VMEM((peers, message, 128), BF16),
            pltpu.VMEM((384, 256), F32),
            dma((6,)),
            dma((5,)),
            dma((5,)),
            dma((peers,)),
            dma((peers,)),
            dma((peers,)),
            dma((peers,)),
        ],
        compiler_params=pltpu.CompilerParams(**params),
        cost_estimate=pl.CostEstimate(
            flops=80_000_000_000, bytes_accessed=8_000_000, transcendentals=0
        ),
        name="mixer",
    )(*arrays)


def sent_together(arrays, axis, dim, along):
    ends, at = ([], 0)
    for a in arrays[:-1]:
        at += a.shape[along]
        ends.append(at)
    both = jnp.concatenate(arrays, axis=along)
    return tuple(jnp.split(lax.all_gather(both, axis, axis=dim, tiled=True), ends, axis=along))


def in_blocks(shard, dim, size):
    before, after = (shard.shape[:dim], shard.shape[dim + 1 :])
    return jnp.moveaxis(shard.reshape(*before, size, -1, *after), dim, 0)


def summed_on_arrival(shard, axis, dim):
    pieces = in_blocks(shard, dim, lax.axis_size(axis))
    arrived = lax.all_to_all(pieces, axis, split_axis=0, concat_axis=0, tiled=True)
    return arrived.astype(jnp.float32).sum(axis=0)


def on_device(
    residual,
    value_projected,
    gate_projected,
    wide_key_rows,
    wide_query_rows,
    narrow_key_rows,
    narrow_query_rows,
    step_before_softplus,
    extra_log_decay,
    log_decay_rate,
    value_kernel,
    wide_key_kernel,
    wide_query_kernel,
    narrow_key_kernel,
    narrow_query_kernel,
    head_norm_gain,
    output_matrix,
    feedforward_norm_gain,
    gate_matrix,
    up_matrix,
    down_matrix,
):
    normed = mixer(
        [
            value_projected,
            wide_key_rows,
            wide_query_rows,
            narrow_key_rows,
            narrow_query_rows,
            gate_projected,
            step_before_softplus,
            extra_log_decay,
            log_decay_rate[None],
            value_kernel,
            wide_key_kernel,
            wide_query_kernel,
            narrow_key_kernel,
            narrow_query_kernel,
            head_norm_gain[None],
        ],
        lax.axis_size("sp"),
    )
    projected = summed_on_arrival(
        jnp.dot(normed, output_matrix, preferred_element_type=jnp.float32).astype(jnp.bfloat16),
        "tp",
        0,
    )
    after_mixer = (residual.astype(jnp.float32) + projected).astype(jnp.bfloat16)
    rows = after_mixer.astype(jnp.float32)
    x_norm = (
        rows
        * lax.rsqrt(jnp.mean(rows * rows, axis=-1, keepdims=True) + 1e-06)
        * feedforward_norm_gain.astype(jnp.float32)
    ).astype(jnp.bfloat16)
    gate_full, up_full, down_full = sent_together((gate_matrix, up_matrix, down_matrix), "sp", 0, 1)
    x_norm, gate_full, up_full, down_full = lax.optimization_barrier(
        (x_norm, gate_full, up_full, down_full)
    )
    piece = lax.all_gather(x_norm, "tp", axis=0, tiled=True)
    gate_values = jnp.dot(piece, gate_full, preferred_element_type=jnp.float32)
    up_values = jnp.dot(piece, up_full, preferred_element_type=jnp.float32)
    hidden = (jax.nn.silu(gate_values) * up_values).astype(jnp.bfloat16)
    channel = summed_on_arrival(
        lax.dot_general(
            hidden, down_full, (((1,), (1,)), ((), ())), preferred_element_type=jnp.float32
        ).astype(jnp.bfloat16),
        "tp",
        0,
    )
    return (after_mixer.astype(jnp.float32) + 0.5 * channel).astype(jnp.bfloat16)


def solution(mesh):
    in_specs = (
        P(("grp", "sp", "tp"), None),
        P(("grp", "sp"), "tp"),
        P(("grp", "sp"), "tp"),
        P(("grp", "sp"), "tp"),
        P(("grp", "sp"), "tp"),
        P(("grp", "sp"), "tp"),
        P(("grp", "sp"), "tp"),
        P(("grp", "sp"), "tp"),
        P(("grp", "sp"), "tp"),
        P("tp"),
        P(None, "tp"),
        P(None, "tp"),
        P(None, "tp"),
        P(None, "tp"),
        P(None, "tp"),
        P("tp"),
        P("tp", None),
        P(),
        P("sp", "tp"),
        P("sp", "tp"),
        P("sp", "tp"),
    )
    out_specs = P(("grp", "sp", "tp"), None)
    return jax.shard_map(
        on_device, mesh=mesh, in_specs=in_specs, out_specs=out_specs, check_vma=False
    )
```

```python
import functools
import jax
import jax.numpy as jnp
from jax import lax
from jax.experimental import pallas as pl
from jax.experimental.pallas import tpu as pltpu
from jax.sharding import PartitionSpec as P

F32 = jnp.float32
BF16 = jnp.bfloat16
MESH = pl.DeviceIdType.MESH
CH = 128
PAD = 16
GROUP_Q = (0, 256, 128, 384)
GROUP_K = (0, 256, 128, 256)
ROW_GROUP = ((0, 128, 0), (128, 256, 2), (256, 320, 1), (320, 384, 3))
HIGH = lax.Precision.HIGHEST


def pair_lanes(columns, head):
    rows = columns.shape[0]
    lane = lax.broadcasted_iota(jnp.int32, (rows, 128), 1)
    return jnp.where(
        lane < 64,
        jnp.broadcast_to(columns[:, head : head + 1], (rows, 128)),
        jnp.broadcast_to(columns[:, head + 1 : head + 2], (rows, 128)),
    )


def quad_lanes(columns, group):
    return jnp.concatenate(
        [pair_lanes(columns, 4 * group), pair_lanes(columns, 4 * group + 2)], axis=1
    )


def silu(x):
    return x / (1.0 + jnp.exp(-x))


def matmul(a, b, dims=((1,), (0,)), precision=None):
    return lax.dot_general(a, b, (dims, ((), ())), preferred_element_type=F32, precision=precision)


def group_of_row(row):
    for low, high, group in ROW_GROUP:
        if low <= row < high:
            return group


def mixer_kernel(
    peers,
    value_ref,
    wk_ref,
    wq_ref,
    nk_ref,
    nq_ref,
    gate_ref,
    step_ref,
    extra_ref,
    rate_ref,
    vker_ref,
    wkker_ref,
    wqker_ref,
    nkker_ref,
    nqker_ref,
    gain_ref,
    normed_ref,
    xpad,
    ubuf,
    kbuf,
    qbuf,
    gbuf,
    rcol,
    qrow,
    total,
    ebuf,
    hbuf,
    ybuf,
    out_msg,
    in_msg,
    out_ret,
    in_ret,
    hent,
    local_sem,
    rim_send,
    rim_recv,
    send_a,
    recv_a,
    send_b,
    recv_b,
):
    length = value_ref.shape[0]
    count = length // CH
    me = lax.axis_index("sp")
    inputs = (value_ref, wk_ref, wq_ref, nk_ref, nq_ref)
    spans = []
    at = 0
    for ref in inputs:
        spans.append((at, at + ref.shape[1]))
        at += ref.shape[1]
    loads = [
        pltpu.make_async_copy(
            ref, xpad.at[pl.ds(PAD, length), pl.ds(low, high - low)], local_sem.at[n]
        )
        for n, (ref, (low, high)) in enumerate(zip(inputs, spans))
    ]
    loads.append(pltpu.make_async_copy(gate_ref, gbuf, local_sem.at[len(inputs)]))
    for load in loads:
        load.start()
    rims = []
    if peers > 1:
        barrier = pltpu.get_barrier_semaphore()
        for offset in range(1, peers):
            pl.semaphore_signal(
                barrier,
                inc=1,
                device_id={"sp": lax.rem(me + offset, peers)},
                device_id_type=MESH,
            )
        pl.semaphore_wait(barrier, peers - 1)
        for n, (ref, (low, high)) in enumerate(zip(inputs, spans)):
            rims.append(
                pltpu.make_async_remote_copy(
                    src_ref=ref.at[pl.ds(length - PAD, PAD)],
                    dst_ref=xpad.at[pl.ds(0, PAD), pl.ds(low, high - low)],
                    send_sem=rim_send.at[n],
                    recv_sem=rim_recv.at[n],
                    device_id={"sp": lax.rem(me + 1, peers)},
                    device_id_type=MESH,
                )
            )
        for rim in rims:
            rim.start()
    for load in loads[:-1]:
        load.wait()

    row_id = lax.broadcasted_iota(jnp.int32, (CH, CH), 0)
    col_id = lax.broadcasted_iota(jnp.int32, (CH, CH), 1)
    lower = row_id >= col_id
    tril = lower.astype(F32)
    triu = (row_id <= col_id).astype(F32)
    eye = (row_id == col_id).astype(F32)
    left = lax.broadcasted_iota(jnp.int32, (CH, 128), 1) < 64
    kernels = (vker_ref, wkker_ref, wqker_ref, nkker_ref, nqker_ref)

    def conv_tile(base, which, tile):
        low = spans[which][0] + 128 * tile
        columns = pl.ds(low, 128)
        before = xpad[pl.ds(base, PAD), columns].astype(F32)[PAD - 8 :]
        here = xpad[pl.ds(base + PAD, CH), columns].astype(F32)
        rows = jnp.concatenate([before, here], axis=0)
        taps = kernels[which][:, 128 * tile : 128 * tile + 128].astype(F32)
        acc = here * taps[3:4]
        for tap in range(3):
            acc = acc + pltpu.roll(rows, 3 - tap, 0)[8:] * taps[tap : tap + 1]
        return silu(acc)

    def first_pass(i, carry):
        c = lax.rem(i + 1, count)
        base = pl.multiple_of(c * CH, CH)

        @pl.when(i == count - 1)
        def _():
            for rim in rims:
                rim.wait()

            @pl.when(me == 0)
            def _():
                xpad[0:PAD, :] = jnp.zeros((PAD, xpad.shape[1]), BF16)

        here = pl.ds(base, CH)
        dt = step_ref[here, :]
        dt = jnp.maximum(dt, 0.0) + jnp.log(1.0 + jnp.exp(-jnp.abs(dt)))
        a = -jnp.exp(rate_ref[...]) * dt + extra_ref[here, :]
        r = matmul(tril, a, precision=HIGH)
        r_row = matmul(a, triu, ((0,), (0,)), HIGH)
        dt_row = matmul(dt, eye, ((0,), (0,)), HIGH)
        rcol[here, :] = r
        qrow[c] = r_row - jnp.log(dt_row)
        end = r[CH - 1 : CH, :]
        total[c] = end
        fade = dt * jnp.exp(end - r)
        for tile in range(2):
            kbuf[here, 128 * tile : 128 * tile + 128] = conv_tile(base, 1, tile).astype(BF16)
            qbuf[here, 128 * tile : 128 * tile + 128] = conv_tile(base, 2, tile).astype(BF16)
        kbuf[here, 256:384] = conv_tile(base, 3, 0).astype(BF16)
        narrow_q = conv_tile(base, 4, 0)
        qbuf[here, 256:384] = jnp.where(left, narrow_q, 0.0).astype(BF16)
        qbuf[here, 384:512] = jnp.where(left, 0.0, narrow_q).astype(BF16)
        for group in range(4):
            parts = []
            for half in range(2):
                pair = 2 * group + half
                u = conv_tile(base, 0, pair).astype(BF16)
                ubuf[here, 128 * pair : 128 * pair + 128] = u
                parts.append((u.astype(F32) * pair_lanes(fade, 2 * pair)).astype(BF16))
            v = jnp.concatenate(parts, axis=1)
            k = kbuf[here, GROUP_K[group] : GROUP_K[group] + 128]
            e = matmul(k, v, ((0,), (0,)))
            if group == 0:
                ebuf[c, 0:128, :] = e
            elif group == 2:
                ebuf[c, 128:256, :] = e
            elif group == 1:
                ebuf[c, 256:320, :] = e[0:64]
            else:
                ebuf[c, 320:384, :] = e[64:128]
        return carry

    lax.fori_loop(0, count, first_pass, 0)

    offsets = [jnp.zeros((1, 16), F32)]
    for c in range(count):
        offsets.append(offsets[-1] + total[c])
    whole = offsets[-1]
    for low, high, group in ROW_GROUP:
        state = jnp.zeros((high - low, 256), F32)
        for c in range(count):
            hbuf[c, low:high, :] = state.astype(BF16)
            state = state * jnp.exp(quad_lanes(total[c], group)) + ebuf[c, low:high, :]
        hent[low:high, :] = state

    if peers > 1:
        per = 384 // (peers // 2)
        wide_log = [quad_lanes(whole, group) for group in range(4)]
        sub = lax.broadcasted_iota(jnp.int32, (8, 128), 0)
        for slot in range(peers):
            z, core = slot // 2, slot % 2
            lanes = slice(128 * core, 128 * core + 128)
            logs = jnp.zeros((8, 128), F32)
            for tile in range(per // 8):
                line = wide_log[group_of_row(per * z + 8 * tile)][:, lanes]
                logs = jnp.where(sub == tile, jnp.broadcast_to(line, (8, 128)), logs)
            body = hent[per * z : per * z + per, lanes]
            out_msg[slot] = jnp.concatenate([body, logs], axis=0).astype(BF16)

        def exchange(source, target, send, recv):
            order = sorted(range(1, peers), key=lambda o: -min(o, peers - o))
            copies = []
            for offset in order:
                to = lax.rem(me + offset, peers)
                copies.append(
                    pltpu.make_async_remote_copy(
                        src_ref=source.at[to],
                        dst_ref=target.at[me],
                        send_sem=send.at[offset],
                        recv_sem=recv.at[offset],
                        device_id={"sp": to},
                        device_id_type=MESH,
                    )
                )
            return copies

        phase_a = exchange(out_msg, in_msg, send_a, recv_a)
        for copy in phase_a:
            copy.start()
        in_msg[me] = out_msg[me]

    for c in range(count):
        here = slice(c * CH, c * CH + CH)
        r = rcol[here, :]
        fade_out = jnp.exp(r)
        for group in range(4):
            q = qbuf[here, GROUP_Q[group] : GROUP_Q[group] + 128]
            k = kbuf[here, GROUP_K[group] : GROUP_K[group] + 128]
            score = matmul(q, k, ((1,), (1,)))
            row = 0 if group == 0 else 128 if group == 2 else 256
            outer = matmul(q, hbuf[c, row : row + 128, :])
            for half in range(2):
                pair = 2 * group + half
                weights = []
                for head in (2 * pair, 2 * pair + 1):
                    gap = jnp.broadcast_to(r[:, head : head + 1], (CH, CH)) - qrow[c, head : head + 1, :]
                    w = score * jnp.exp(jnp.where(lower, gap, -jnp.inf))
                    weights.append(w.astype(BF16))
                u = ubuf[here, 128 * pair : 128 * pair + 128].astype(F32)
                both = jnp.concatenate(
                    [jnp.where(left, u, 0.0).astype(BF16), jnp.where(left, 0.0, u).astype(BF16)],
                    axis=0,
                )
                inner = matmul(jnp.concatenate(weights, axis=1), both)
                ybuf[here, 128 * pair : 128 * pair + 128] = (
                    inner + outer[:, 128 * half : 128 * half + 128] * pair_lanes(fade_out, 2 * pair)
                )

    if peers > 1:
        for copy in phase_a:
            copy.wait()
        tiles = per // 8
        state = [jnp.zeros((8, 128), F32) for _ in range(tiles)]
        for source in range(peers):
            out_ret[source] = jnp.concatenate(
                state + [jnp.zeros((8, 128), F32)], axis=0
            ).astype(BF16)
            message = in_msg[source].astype(F32)
            for tile in range(tiles):
                decay = jnp.exp(message[per + tile : per + tile + 1, :])
                state[tile] = state[tile] * decay + message[8 * tile : 8 * tile + 8, :]
        phase_b = exchange(out_ret, in_ret, send_b, recv_b)
        for copy in phase_b:
            copy.start()
        in_ret[me] = out_ret[me]

    loads[-1].wait()
    if peers > 1:
        for copy in phase_b:
            copy.wait()
        for slot in range(peers):
            z, core = slot // 2, slot % 2
            hent[per * z : per * z + per, 128 * core : 128 * core + 128] = in_ret[slot].astype(
                F32
            )[:per]
    ones = (
        (row_id < 64) == (col_id < 64)
    ).astype(BF16)

    for c in range(count):
        here = slice(c * CH, c * CH + CH)
        reach = jnp.exp(rcol[here, :] + offsets[c])
        for group in range(4):
            if peers > 1:
                q = qbuf[here, GROUP_Q[group] : GROUP_Q[group] + 128]
                row = 0 if group == 0 else 128 if group == 2 else 256
                entered = matmul(q, hent[row : row + 128, :].astype(BF16))
            for half in range(2):
                pair = 2 * group + half
                lanes = slice(128 * pair, 128 * pair + 128)
                y = ybuf[here, lanes]
                if peers > 1:
                    y = y + entered[:, 128 * half : 128 * half + 128] * pair_lanes(reach, 2 * pair)
                gated = y * silu(gbuf[here, lanes].astype(F32))
                square = matmul((gated * gated).astype(BF16), ones)
                scale = lax.rsqrt(square * (1.0 / 64.0) + 1e-06)
                normed_ref[here, lanes] = (
                    gated * scale * gain_ref[:, lanes].astype(F32)
                ).astype(BF16)


def mixer(arrays, peers):
    length = arrays[0].shape[0]
    width = sum(a.shape[1] for a in arrays[:5])
    count = length // CH
    channels = arrays[0].shape[1]
    message = 384 // max(peers // 2, 1) + 8
    any_space = pl.BlockSpec(memory_space=pl.ANY)
    vmem = pl.BlockSpec(memory_space=pltpu.VMEM)
    dma = pltpu.SemaphoreType.DMA
    params = dict(vmem_limit_bytes=56 * 1024 * 1024)
    if peers > 1:
        params.update(collective_id=1, has_side_effects=True)
    return pl.pallas_call(
        functools.partial(mixer_kernel, peers),
        out_shape=jax.ShapeDtypeStruct((length, channels), BF16),
        in_specs=[any_space] * 6 + [vmem] * 9,
        out_specs=vmem,
        scratch_shapes=[
            pltpu.VMEM((PAD + length, width), BF16),
            pltpu.VMEM((length, channels), BF16),
            pltpu.VMEM((length, 384), BF16),
            pltpu.VMEM((length, 512), BF16),
            pltpu.VMEM((length, channels), BF16),
            pltpu.VMEM((length, 16), F32),
            pltpu.VMEM((count, 16, CH), F32),
            pltpu.VMEM((count, 1, 16), F32),
            pltpu.VMEM((count, 384, 256), F32),
            pltpu.VMEM((count, 384, 256), BF16),
            pltpu.VMEM((length, channels), F32),
            pltpu.VMEM((peers, message, 128), BF16),
            pltpu.VMEM((peers, message, 128), BF16),
            pltpu.VMEM((peers, message, 128), BF16),
            pltpu.VMEM((peers, message, 128), BF16),
            pltpu.VMEM((384, 256), F32),
            dma((6,)),
            dma((5,)),
            dma((5,)),
            dma((peers,)),
            dma((peers,)),
            dma((peers,)),
            dma((peers,)),
        ],
        compiler_params=pltpu.CompilerParams(**params),
        cost_estimate=pl.CostEstimate(
            flops=80_000_000_000, bytes_accessed=8_000_000, transcendentals=0
        ),
        name="mixer",
    )(*arrays)


ROW_PARTS = 2


def silu_gate(x):
    return x / (1.0 + jnp.exp(-x))


class Reducer:
    def __init__(self, axis, buffers, send, recv):
        self.me = lax.axis_index(axis)
        self.right = lax.rem(self.me + 1, 4)
        self.left = lax.rem(self.me + 3, 4)
        self.far = lax.rem(self.me + 2, 4)
        self.axis = axis
        (self.blocks, self.own, self.relay_r, self.relay_l, self.comb_r, self.comb_l,
         self.from_l, self.from_r) = buffers
        self.send, self.recv = send, recv
        self.rows = self.own.shape[0] // ROW_PARTS
        self.half = self.own.shape[1] // 2

    def copy(self, part, index, source, target, to):
        return pltpu.make_async_remote_copy(
            src_ref=source,
            dst_ref=target,
            send_sem=self.send.at[part, index],
            recv_sem=self.recv.at[part, index],
            device_id={self.axis: to},
            device_id_type=MESH,
        )

    def leg(self, part, index):
        rows = pl.ds(part * self.rows, self.rows)
        a, b = pl.ds(0, self.half), pl.ds(self.half, self.half)
        source, target = (
            (self.blocks.at[0, rows, a], self.relay_r.at[rows]),
            (self.blocks.at[1, rows, b], self.from_l.at[rows, b]),
            (self.comb_r.at[rows], self.from_l.at[rows, a]),
            (self.blocks.at[0, rows, b], self.relay_l.at[rows]),
            (self.blocks.at[2, rows, a], self.from_r.at[rows, a]),
            (self.comb_l.at[rows], self.from_r.at[rows, b]),
        )[index]
        return self.copy(part, index, source, target, self.right if index < 3 else self.left)

    def combine(self, part):
        step = 32

        for n, block, low, relay, comb in (
            (0, 1, 0, self.relay_r, self.comb_r),
            (3, 2, self.half, self.relay_l, self.comb_l),
        ):
            self.leg(part, n).wait_recv()

            def body(i, carry, block=block, low=low, relay=relay, comb=comb):
                rows = pl.ds(pl.multiple_of(part * self.rows + i * step, 16), step)
                comb[rows, :] = (
                    self.blocks[block, rows, low : low + self.half].astype(F32)
                    + relay[rows, :].astype(F32)
                ).astype(BF16)
                return carry

            lax.fori_loop(0, self.rows // step, body, 0)
            self.leg(part, n + 2).start()

    def wait_final(self, part):
        for n in (1, 2, 4, 5):
            self.leg(part, n).wait_recv()

    def wait_sends(self):
        for part in range(ROW_PARTS):
            for n in range(6):
                self.leg(part, n).wait_send()

    def total(self, rows):
        return (
            self.own[rows, :]
            + self.from_l[rows, :].astype(F32)
            + self.from_r[rows, :].astype(F32)
        )


def greet(axis, others):
    barrier = pltpu.get_barrier_semaphore()
    for other in others:
        pl.semaphore_signal(barrier, inc=1, device_id={axis: other}, device_id_type=MESH)
    pl.semaphore_wait(barrier, len(others))


def reducer_scratch(rows, width):
    half = width // 2
    dma = pltpu.SemaphoreType.DMA
    return [
        pltpu.VMEM((3, rows, width), BF16),
        pltpu.VMEM((rows, width), F32),
        pltpu.VMEM((rows, half), BF16),
        pltpu.VMEM((rows, half), BF16),
        pltpu.VMEM((rows, half), BF16),
        pltpu.VMEM((rows, half), BF16),
        pltpu.VMEM((rows, width), BF16),
        pltpu.VMEM((rows, width), BF16),
        dma((ROW_PARTS, 6)),
        dma((ROW_PARTS, 6)),
    ]


def project_kernel(
    normed_ref, weight_ref, residual_ref, gain_ref, x_ref, after_ref, *scratch
):
    buffers, (send, recv, gsend, grecv) = scratch[:8], scratch[8:]
    red = Reducer("tp", buffers, send, recv)
    blocks, own = buffers[0], buffers[1]
    rows, width = own.shape
    half = width // 2
    greet("tp", (red.right, red.left))

    def make(owner, slot):
        source = pl.ds(pl.multiple_of(owner * rows, 64), rows)

        def body(j, carry):
            columns = pl.ds(pl.multiple_of(j * 256, 256), 256)
            product = matmul(normed_ref[source, :], weight_ref[:, columns])
            if slot is None:
                own[:, columns] = product
            else:
                blocks[slot, :, columns] = product.astype(BF16)
            return carry

        lax.fori_loop(0, width // 256, body, 0)

    make(red.far, 0)
    red.leg(0, 0).start()
    red.leg(0, 3).start()
    make(red.right, 1)
    red.leg(0, 1).start()
    make(red.left, 2)
    red.leg(0, 4).start()
    make(red.me, None)

    part_rows = red.rows

    def spread(part, index, owner, low, to):
        where = x_ref.at[
            pl.ds(pl.multiple_of(owner * rows + part * part_rows, 32), part_rows),
            pl.ds(low, half),
        ]
        return pltpu.make_async_remote_copy(
            src_ref=where,
            dst_ref=where,
            send_sem=gsend.at[part, index],
            recv_sem=grecv.at[part, index],
            device_id={"tp": to},
            device_id_type=MESH,
        )

    def leaving(part, index):
        owner = (red.me, red.me, red.left, red.me, red.me, red.right)[index]
        low = (0, half, 0, half, 0, half)[index]
        return spread(part, index, owner, low, red.right if index < 3 else red.left)

    def coming(part, index):
        owner = (red.left, red.left, red.far, red.right, red.right, red.far)[index]
        low = (0, half, 0, half, 0, half)[index]
        return spread(part, index, owner, low, red.right if index < 3 else red.left)

    def finish(part):
        red.wait_final(part)

        def body(i, carry):
            at = part * part_rows + i * 16
            here = pl.ds(pl.multiple_of(at, 16), 16)
            after = (residual_ref[here, :].astype(F32) + red.total(here)).astype(BF16)
            after_ref[here, :] = after
            x = after.astype(F32)
            scale = lax.rsqrt(jnp.mean(x * x, axis=1, keepdims=True) + 1e-06)
            x_ref[pl.ds(pl.multiple_of(red.me * rows + at, 16), 16), :] = (
                x * scale * gain_ref[...].astype(F32)
            ).astype(BF16)
            return carry

        lax.fori_loop(0, part_rows // 16, body, 0)
        for n in (0, 3, 1, 4):
            leaving(part, n).start()

    def pass_on(part):
        for n in (0, 3):
            coming(part, n).wait_recv()
            leaving(part, n + 2).start()

    red.combine(0)
    for n in (0, 3, 1, 4):
        red.leg(1, n).start()
    finish(0)
    red.combine(1)
    pass_on(0)
    finish(1)
    pass_on(1)
    for part in range(ROW_PARTS):
        for n in (1, 2, 4, 5):
            coming(part, n).wait_recv()
        for n in range(6):
            leaving(part, n).wait_send()
    red.wait_sends()


def project(normed, weight, residual, gain):
    rows, width = residual.shape
    vmem = pl.BlockSpec(memory_space=pltpu.VMEM)
    dma = pltpu.SemaphoreType.DMA
    return pl.pallas_call(
        project_kernel,
        out_shape=(
            jax.ShapeDtypeStruct((4 * rows, width), BF16),
            jax.ShapeDtypeStruct((rows, width), BF16),
        ),
        in_specs=[vmem] * 4,
        out_specs=(vmem, vmem),
        scratch_shapes=reducer_scratch(rows, width)
        + [dma((ROW_PARTS, 6)), dma((ROW_PARTS, 6))],
        compiler_params=pltpu.CompilerParams(
            collective_id=2, has_side_effects=True, vmem_limit_bytes=40 * 1024 * 1024
        ),
        cost_estimate=pl.CostEstimate(
            flops=80_000_000_000, bytes_accessed=8_000_000, transcendentals=0
        ),
        name="project",
    )(normed, weight, residual, gain)


def feed_kernel(x_ref, stored_ref, after_ref, out_ref, *scratch):
    buffers, (send, recv, hidden, weight_ref, load_sem) = scratch[:8], scratch[8:]
    red = Reducer("tp", buffers, send, recv)
    blocks, own = buffers[0], buffers[1]
    rows, width = own.shape
    units = weight_ref.shape[1] // 3
    tiles = units // 256

    def load(index):
        if isinstance(index, int) and index == 2 * tiles:
            columns = pl.ds(2 * units, units)
        else:
            columns = pl.ds(pl.multiple_of(index * 256, 256), 256)
        return pltpu.make_async_copy(
            stored_ref.at[:, columns], weight_ref.at[:, columns], load_sem.at[index]
        )

    for j in range(tiles):
        load(j).start()
        load(tiles + j).start()
    load(2 * tiles).start()
    greet("tp", (red.right, red.left))

    def make(owner, slot, first=False):
        source = pl.ds(pl.multiple_of(owner * rows, 64), rows)

        def inner(j, carry):
            low = pl.multiple_of(j * 256, 256)
            if first:
                load(j).wait()
                load(tiles + j).wait()
            x = x_ref[source, :]
            gate = matmul(x, weight_ref[:, pl.ds(low, 256)])
            up = matmul(x, weight_ref[:, pl.ds(pl.multiple_of(units + low, 256), 256)])
            hidden[:, pl.ds(low, 256)] = (silu_gate(gate) * up).astype(BF16)
            return carry

        lax.fori_loop(0, tiles, inner, 0)
        if first:
            load(2 * tiles).wait()

        def body(j, carry):
            columns = pl.ds(pl.multiple_of(j * 256, 256), 256)
            product = matmul(
                hidden[...], weight_ref[columns, 2 * units : 3 * units], ((1,), (1,))
            )
            if slot is None:
                own[:, columns] = product
            else:
                blocks[slot, :, columns] = product.astype(BF16)
            return carry

        lax.fori_loop(0, width // 256, body, 0)

    make(red.far, 0, True)
    red.leg(0, 0).start()
    red.leg(0, 3).start()
    make(red.right, 1)
    red.leg(0, 1).start()
    make(red.left, 2)
    red.leg(0, 4).start()
    red.combine(0)
    for n in (0, 3, 1, 4):
        red.leg(1, n).start()
    make(red.me, None)

    def finish(part):
        red.wait_final(part)

        def body(i, carry):
            here = pl.ds(pl.multiple_of(part * red.rows + i * 16, 16), 16)
            out_ref[here, :] = (
                after_ref[here, :].astype(F32) + 0.5 * red.total(here)
            ).astype(BF16)
            return carry

        lax.fori_loop(0, red.rows // 16, body, 0)

    finish(0)
    red.combine(1)
    finish(1)
    red.wait_sends()


def feed(x, weight, after):
    rows, width = after.shape
    units = weight.shape[1] // 3
    vmem = pl.BlockSpec(memory_space=pltpu.VMEM)
    return pl.pallas_call(
        feed_kernel,
        out_shape=jax.ShapeDtypeStruct((rows, width), BF16),
        in_specs=[vmem, pl.BlockSpec(memory_space=pl.ANY), vmem],
        out_specs=vmem,
        scratch_shapes=reducer_scratch(rows, width)
        + [
            pltpu.VMEM((rows, units), BF16),
            pltpu.VMEM(weight.shape, BF16),
            pltpu.SemaphoreType.DMA((2 * units // 256 + 1,)),
        ],
        compiler_params=pltpu.CompilerParams(
            collective_id=3, has_side_effects=True, vmem_limit_bytes=48 * 1024 * 1024
        ),
        cost_estimate=pl.CostEstimate(
            flops=40_000_000_000, bytes_accessed=8_000_000, transcendentals=0
        ),
        name="feed",
    )(x, weight, after)


def on_device(
    residual,
    value_projected,
    gate_projected,
    wide_key_rows,
    wide_query_rows,
    narrow_key_rows,
    narrow_query_rows,
    step_before_softplus,
    extra_log_decay,
    log_decay_rate,
    value_kernel,
    wide_key_kernel,
    wide_query_kernel,
    narrow_key_kernel,
    narrow_query_kernel,
    head_norm_gain,
    output_matrix,
    feedforward_norm_gain,
    gate_matrix,
    up_matrix,
    down_matrix,
):
    normed = mixer(
        [
            value_projected,
            wide_key_rows,
            wide_query_rows,
            narrow_key_rows,
            narrow_query_rows,
            gate_projected,
            step_before_softplus,
            extra_log_decay,
            log_decay_rate[None],
            value_kernel,
            wide_key_kernel,
            wide_query_kernel,
            narrow_key_kernel,
            narrow_query_kernel,
            head_norm_gain[None],
        ],
        lax.axis_size("sp"),
    )
    x_full, after_mixer = project(
        normed, output_matrix, residual, feedforward_norm_gain[None]
    )
    shard = jnp.concatenate((gate_matrix, up_matrix, down_matrix), axis=1)
    weights = lax.all_gather(shard, "sp", axis=0, tiled=True)
    return feed(x_full, weights, after_mixer)


def solution(mesh):
    in_specs = (
        P(("grp", "sp", "tp"), None),
        P(("grp", "sp"), "tp"),
        P(("grp", "sp"), "tp"),
        P(("grp", "sp"), "tp"),
        P(("grp", "sp"), "tp"),
        P(("grp", "sp"), "tp"),
        P(("grp", "sp"), "tp"),
        P(("grp", "sp"), "tp"),
        P(("grp", "sp"), "tp"),
        P("tp"),
        P(None, "tp"),
        P(None, "tp"),
        P(None, "tp"),
        P(None, "tp"),
        P(None, "tp"),
        P("tp"),
        P("tp", None),
        P(),
        P("sp", "tp"),
        P("sp", "tp"),
        P("sp", "tp"),
    )
    out_specs = P(("grp", "sp", "tp"), None)
    return jax.shard_map(
        on_device, mesh=mesh, in_specs=in_specs, out_specs=out_specs, check_vma=False
    )
```

```python
import functools
import jax
import jax.numpy as jnp
from jax import lax
from jax.experimental import pallas as pl
from jax.experimental.pallas import tpu as pltpu
from jax.sharding import PartitionSpec as P

F32 = jnp.float32
BF16 = jnp.bfloat16
MESH = pl.DeviceIdType.MESH
CH = 128
PAD = 16
PIECE = 48
GROUP_Q = (0, 256, 128, 384)
GROUP_K = (0, 256, 128, 256)
ROW_GROUP = ((0, 128, 0), (128, 256, 2), (256, 320, 1), (320, 384, 3))
HIGH = lax.Precision.HIGHEST


def pair_lanes(columns, head):
    rows = columns.shape[0]
    lane = lax.broadcasted_iota(jnp.int32, (rows, 128), 1)
    return jnp.where(
        lane < 64,
        jnp.broadcast_to(columns[:, head : head + 1], (rows, 128)),
        jnp.broadcast_to(columns[:, head + 1 : head + 2], (rows, 128)),
    )


def quad_lanes(columns, group):
    return jnp.concatenate(
        [pair_lanes(columns, 4 * group), pair_lanes(columns, 4 * group + 2)], axis=1
    )


def silu(x):
    return x / (1.0 + jnp.exp(-x))


def matmul(a, b, dims=((1,), (0,)), precision=None):
    return lax.dot_general(a, b, (dims, ((), ())), preferred_element_type=F32, precision=precision)


def group_of_row(row):
    for low, high, group in ROW_GROUP:
        if low <= row < high:
            return group


def mixer_part(
    peers,
    service,
    value_ref,
    wk_ref,
    wq_ref,
    nk_ref,
    nq_ref,
    gate_ref,
    step_ref,
    extra_ref,
    rate_ref,
    vker_ref,
    wkker_ref,
    wqker_ref,
    nkker_ref,
    nqker_ref,
    gain_ref,
    normed_ref,
    xpad,
    ubuf,
    kbuf,
    qbuf,
    gbuf,
    rcol,
    qrow,
    total,
    ebuf,
    hbuf,
    ybuf,
    hent,
    entered_ref,
    half_out,
    half_in,
    chain_in,
    chain_out,
    local_sem,
    rim_send,
    rim_recv,
    swap_send,
    swap_recv,
    chain_send,
    chain_recv,
):
    length = value_ref.shape[0]
    count = length // CH
    me = lax.axis_index("sp")
    inputs = (value_ref, wk_ref, wq_ref, nk_ref, nq_ref)
    spans = []
    at = 0
    for ref in inputs:
        spans.append((at, at + ref.shape[1]))
        at += ref.shape[1]
    loads = [
        pltpu.make_async_copy(
            ref, xpad.at[pl.ds(PAD, length), pl.ds(low, high - low)], local_sem.at[n]
        )
        for n, (ref, (low, high)) in enumerate(zip(inputs, spans))
    ]
    loads.append(pltpu.make_async_copy(gate_ref, gbuf, local_sem.at[len(inputs)]))
    for load in loads:
        load.start()
    core = lax.rem(me, 2)
    chip = me // 2
    chips = peers // 2
    partner = me + 1 - 2 * core

    def send_to(peer, source, target, send, recv):
        return pltpu.make_async_remote_copy(
            src_ref=source,
            dst_ref=target,
            send_sem=send,
            recv_sem=recv,
            device_id={"sp": peer},
            device_id_type=MESH,
        )

    def rim(n):
        low, high = spans[n]
        return send_to(
            lax.rem(me + 1, peers),
            inputs[n].at[pl.ds(length - PAD, PAD)],
            xpad.at[pl.ds(0, PAD), pl.ds(low, high - low)],
            rim_send.at[n],
            rim_recv.at[n],
        )

    greet_all(me, peers, service.reply)
    service.open()

    @pl.when(me < peers - 1)
    def _():
        for n in range(len(inputs)):
            rim(n).start()

    for load in loads[:-1]:
        load.wait()

    row_id = lax.broadcasted_iota(jnp.int32, (CH, CH), 0)
    col_id = lax.broadcasted_iota(jnp.int32, (CH, CH), 1)
    lower = row_id >= col_id
    tril = lower.astype(F32)
    triu = (row_id <= col_id).astype(F32)
    eye = (row_id == col_id).astype(F32)
    left = lax.broadcasted_iota(jnp.int32, (CH, 128), 1) < 64
    diagonal = lax.broadcasted_iota(jnp.int32, (16, 16), 0) == lax.broadcasted_iota(
        jnp.int32, (16, 16), 1
    )
    rate = -jnp.sum(
        jnp.where(diagonal, jnp.broadcast_to(jnp.exp(rate_ref[...]), (16, 16)), 0.0),
        axis=1,
        keepdims=True,
    )
    kernels = (vker_ref, wkker_ref, wqker_ref, nkker_ref, nqker_ref)

    def conv_tile(base, which, tile):
        low = spans[which][0] + 128 * tile
        columns = pl.ds(low, 128)
        before = xpad[pl.ds(base, PAD), columns].astype(F32)[PAD - 8 :]
        here = xpad[pl.ds(base + PAD, CH), columns].astype(F32)
        rows = jnp.concatenate([before, here], axis=0)
        taps = kernels[which][:, 128 * tile : 128 * tile + 128].astype(F32)
        acc = here * taps[3:4]
        for tap in range(3):
            acc = acc + pltpu.roll(rows, 3 - tap, 0)[8:] * taps[tap : tap + 1]
        return silu(acc)

    def first_pass(i, carry):
        c = lax.rem(i + 1, count)
        base = pl.multiple_of(c * CH, CH)

        @pl.when(i == count - 1)
        def _():
            @pl.when(me > 0)
            def _():
                for n in range(len(inputs)):
                    rim(n).wait_recv()

            @pl.when(me == 0)
            def _():
                xpad[0:PAD, :] = jnp.zeros((PAD, xpad.shape[1]), BF16)

        here = pl.ds(base, CH)
        dt_row = step_ref[:, here]
        dt_row = jnp.maximum(dt_row, 0.0) + jnp.log(1.0 + jnp.exp(-jnp.abs(dt_row)))
        a = rate * dt_row + extra_ref[:, here]
        r = matmul(tril, a, ((1,), (1,)), HIGH)
        r_row = matmul(a, triu, precision=HIGH)
        dt = matmul(eye, dt_row, ((1,), (1,)), HIGH)
        rcol[here, :] = r
        qrow[c] = r_row - jnp.log(dt_row)
        end = r[CH - 1 : CH, :]
        total[c] = end
        fade = dt * jnp.exp(end - r)
        for tile in range(2):
            kbuf[here, 128 * tile : 128 * tile + 128] = conv_tile(base, 1, tile).astype(BF16)
            qbuf[here, 128 * tile : 128 * tile + 128] = conv_tile(base, 2, tile).astype(BF16)
        kbuf[here, 256:384] = conv_tile(base, 3, 0).astype(BF16)
        narrow_q = conv_tile(base, 4, 0)
        qbuf[here, 256:384] = jnp.where(left, narrow_q, 0.0).astype(BF16)
        qbuf[here, 384:512] = jnp.where(left, 0.0, narrow_q).astype(BF16)
        for group in range(4):
            parts = []
            for half in range(2):
                pair = 2 * group + half
                u = conv_tile(base, 0, pair).astype(BF16)
                ubuf[here, 128 * pair : 128 * pair + 128] = u
                parts.append((u.astype(F32) * pair_lanes(fade, 2 * pair)).astype(BF16))
            v = jnp.concatenate(parts, axis=1)
            k = kbuf[here, GROUP_K[group] : GROUP_K[group] + 128]
            e = matmul(k, v, ((0,), (0,)))
            if group == 0:
                ebuf[c, 0:128, :] = e
            elif group == 2:
                ebuf[c, 128:256, :] = e
            elif group == 1:
                ebuf[c, 256:320, :] = e[0:64]
            else:
                ebuf[c, 320:384, :] = e[64:128]
        service.run(20 + 14 * i, 34 + 14 * i)
        return carry

    lax.fori_loop(0, count, first_pass, 0)

    offsets = [jnp.zeros((1, 16), F32)]
    for c in range(count):
        offsets.append(offsets[-1] + total[c])
    whole = offsets[-1]
    for low, high, group in ROW_GROUP:
        state = jnp.zeros((high - low, 256), F32)
        for c in range(count):
            hbuf[c, low:high, :] = state.astype(BF16)
            state = state * jnp.exp(quad_lanes(total[c], group)) + ebuf[c, low:high, :]
        hent[low:high, :] = state

    log_total = [quad_lanes(whole, group) for group in range(4)]
    sub = lax.broadcasted_iota(jnp.int32, (16, 256), 0)
    swap = send_to(partner, half_out, half_in, swap_send.at[0], swap_recv.at[0])

    @pl.when(core == 0)
    def _():
        half_out[0:384, :] = hent[...].astype(BF16)
        lines = jnp.zeros((16, 256), F32)
        for group in range(4):
            lines = jnp.where(
                sub == group, jnp.broadcast_to(log_total[group], (16, 256)), lines
            )
        half_out[384:400, :] = lines.astype(BF16)
        swap.start()

    def second_pass(c, start):
        here = pl.ds(pl.multiple_of(c * CH, CH), CH)
        r = rcol[here, :]
        fade_out = jnp.exp(r)
        for group in range(4):
            q = qbuf[here, GROUP_Q[group] : GROUP_Q[group] + 128]
            k = kbuf[here, GROUP_K[group] : GROUP_K[group] + 128]
            score = matmul(q, k, ((1,), (1,)))
            row = 0 if group == 0 else 128 if group == 2 else 256
            outer = matmul(q, hbuf[c, row : row + 128, :])
            for half in range(2):
                pair = 2 * group + half
                weights = []
                for head in (2 * pair, 2 * pair + 1):
                    gap = jnp.broadcast_to(r[:, head : head + 1], (CH, CH)) - qrow[c, head : head + 1, :]
                    w = score * jnp.exp(jnp.where(lower, gap, -jnp.inf))
                    weights.append(w.astype(BF16))
                u = ubuf[here, 128 * pair : 128 * pair + 128].astype(F32)
                both = jnp.concatenate(
                    [jnp.where(left, u, 0.0).astype(BF16), jnp.where(left, 0.0, u).astype(BF16)],
                    axis=0,
                )
                inner = matmul(jnp.concatenate(weights, axis=1), both)
                ybuf[here, 128 * pair : 128 * pair + 128] = (
                    inner + outer[:, 128 * half : 128 * half + 128] * pair_lanes(fade_out, 2 * pair)
                )
        service.run(start + 11 * c, start + 11 * c + 11)
        return start

    early = jnp.minimum(count, 1 + chip // 2)
    service.run(20 + 14 * count, 120)
    lax.fori_loop(0, early, second_pass, 120)

    def link(piece):
        rows = pl.ds(piece * PIECE, PIECE)
        return send_to(
            lax.rem(me + 2, peers),
            chain_out.at[rows],
            chain_in.at[rows],
            chain_send.at[piece],
            chain_recv.at[piece],
        )

    hand = send_to(partner, chain_in, entered_ref, swap_send.at[1], swap_recv.at[1])

    @pl.when(core == 1)
    def _():
        swap.wait_recv()
        lines = half_in[384:400, :].astype(F32)
        fade_0 = [jnp.exp(lines[group : group + 1]) for group in range(4)]
        fade_1 = [jnp.exp(line) for line in log_total]

        @pl.when(chip == 0)
        def _():
            chain_in[...] = jnp.zeros_like(chain_in)

        for piece in range(384 // PIECE):

            @pl.when(chip > 0)
            def _():
                link(piece).wait_recv()

            for at in range(piece * PIECE, piece * PIECE + PIECE, 16):
                group = group_of_row(at)
                rows = slice(at, at + 16)
                second = (
                    chain_in[rows, :].astype(F32) * fade_0[group] + half_in[rows, :].astype(F32)
                )
                chain_out[rows, :] = (second * fade_1[group] + hent[rows, :]).astype(BF16)
                entered_ref[rows, :] = second.astype(BF16)

            @pl.when(chip < chips - 1)
            def _():
                link(piece).start()

        hand.start()

    service.run(120 + 11 * early, 130 + 6 * chip)
    lax.fori_loop(early, count, second_pass, 130 + 6 * chip - 11 * early)
    at = 130 + 6 * chip + 11 * (count - early)
    loads[-1].wait()

    @pl.when(core == 0)
    def _():
        swap.wait_send()
        hand.wait_recv()

    @pl.when(core == 1)
    def _():
        hand.wait_send()

    @pl.when((chip < chips - 1) & (core == 1))
    def _():
        for piece in range(384 // PIECE):
            link(piece).wait_send()

    @pl.when(me < peers - 1)
    def _():
        for n in range(len(inputs)):
            rim(n).wait_send()

    ones = (
        (row_id < 64) == (col_id < 64)
    ).astype(BF16)

    for c in range(count):
        here = slice(c * CH, c * CH + CH)
        reach = jnp.exp(rcol[here, :] + offsets[c])
        for group in range(4):
            q = qbuf[here, GROUP_Q[group] : GROUP_Q[group] + 128]
            row = 0 if group == 0 else 128 if group == 2 else 256
            entered = matmul(q, entered_ref[row : row + 128, :])
            for half in range(2):
                pair = 2 * group + half
                lanes = slice(128 * pair, 128 * pair + 128)
                y = ybuf[here, lanes]
                y = y + entered[:, 128 * half : 128 * half + 128] * pair_lanes(reach, 2 * pair)
                gated = y * silu(gbuf[here, lanes].astype(F32))
                square = matmul((gated * gated).astype(BF16), ones)
                scale = lax.rsqrt(square * (1.0 / 64.0) + 1e-06)
                normed_ref[here, lanes] = (
                    gated * scale * gain_ref[:, lanes].astype(F32)
                ).astype(BF16)
        service.run(at, at + 6)
        at = at + 6
    return at


ROW_PARTS = 2


def silu_gate(x):
    return x / (1.0 + jnp.exp(-x))


class Reducer:
    def __init__(self, axis, buffers, send, recv):
        self.me = lax.axis_index(axis)
        self.right = lax.rem(self.me + 1, 4)
        self.left = lax.rem(self.me + 3, 4)
        self.far = lax.rem(self.me + 2, 4)
        self.axis = axis
        (self.blocks, self.own, self.relay_r, self.relay_l, self.comb_r, self.comb_l,
         self.from_l, self.from_r) = buffers
        self.send, self.recv = send, recv
        self.rows = self.own.shape[0] // ROW_PARTS
        self.half = self.own.shape[1] // 2

    def copy(self, part, index, source, target, to):
        return pltpu.make_async_remote_copy(
            src_ref=source,
            dst_ref=target,
            send_sem=self.send.at[part, index],
            recv_sem=self.recv.at[part, index],
            device_id={self.axis: to},
            device_id_type=MESH,
        )

    def leg(self, part, index):
        rows = pl.ds(part * self.rows, self.rows)
        a, b = pl.ds(0, self.half), pl.ds(self.half, self.half)
        source, target = (
            (self.blocks.at[0, rows, a], self.relay_r.at[rows]),
            (self.blocks.at[1, rows, b], self.from_l.at[rows, b]),
            (self.comb_r.at[rows], self.from_l.at[rows, a]),
            (self.blocks.at[0, rows, b], self.relay_l.at[rows]),
            (self.blocks.at[2, rows, a], self.from_r.at[rows, a]),
            (self.comb_l.at[rows], self.from_r.at[rows, b]),
        )[index]
        return self.copy(part, index, source, target, self.right if index < 3 else self.left)

    def combine(self, part):
        step = 32

        for n, block, low, relay, comb in (
            (0, 1, 0, self.relay_r, self.comb_r),
            (3, 2, self.half, self.relay_l, self.comb_l),
        ):
            self.leg(part, n).wait_recv()

            def body(i, carry, block=block, low=low, relay=relay, comb=comb):
                rows = pl.ds(pl.multiple_of(part * self.rows + i * step, 16), step)
                comb[rows, :] = (
                    self.blocks[block, rows, low : low + self.half].astype(F32)
                    + relay[rows, :].astype(F32)
                ).astype(BF16)
                return carry

            lax.fori_loop(0, self.rows // step, body, 0)
            self.leg(part, n + 2).start()

    def wait_final(self, part):
        for n in (1, 2, 4, 5):
            self.leg(part, n).wait_recv()

    def wait_sends(self):
        for part in range(ROW_PARTS):
            for n in range(6):
                self.leg(part, n).wait_send()

    def total(self, rows):
        return (
            self.own[rows, :]
            + self.from_l[rows, :].astype(F32)
            + self.from_r[rows, :].astype(F32)
        )


def reducer_scratch(rows, width):
    half = width // 2
    dma = pltpu.SemaphoreType.DMA
    return [
        pltpu.VMEM((3, rows, width), BF16),
        pltpu.VMEM((rows, width), F32),
        pltpu.VMEM((rows, half), BF16),
        pltpu.VMEM((rows, half), BF16),
        pltpu.VMEM((rows, half), BF16),
        pltpu.VMEM((rows, half), BF16),
        pltpu.VMEM((rows, width), BF16),
        pltpu.VMEM((rows, width), BF16),
        dma((ROW_PARTS, 6)),
        dma((ROW_PARTS, 6)),
    ]


def project_part(
    service, at, normed_ref, weight_ref, residual_ref, gain_ref, x_ref, after_ref, *scratch
):
    buffers, (send, recv, gsend, grecv) = scratch[:8], scratch[8:]
    red = Reducer("tp", buffers, send, recv)
    blocks, own = buffers[0], buffers[1]
    rows, width = own.shape
    half = width // 2

    def make(owner, slot):
        source = pl.ds(pl.multiple_of(owner * rows, 64), rows)

        def body(j, carry):
            columns = pl.ds(pl.multiple_of(j * 256, 256), 256)
            product = matmul(normed_ref[source, :], weight_ref[:, columns])
            if slot is None:
                own[:, columns] = product
            else:
                blocks[slot, :, columns] = product.astype(BF16)
            return carry

        lax.fori_loop(0, width // 256, body, 0)

    make(red.far, 0)
    red.leg(0, 0).start()
    red.leg(0, 3).start()
    service.run(at, at + 20)
    make(red.right, 1)
    red.leg(0, 1).start()
    make(red.left, 2)
    red.leg(0, 4).start()
    make(red.me, None)
    service.open_last()
    service.run(at + 20, at + 65)

    part_rows = red.rows

    def spread(part, index, owner, low, to):
        where = x_ref.at[
            pl.ds(pl.multiple_of(owner * rows + part * part_rows, 32), part_rows),
            pl.ds(low, half),
        ]
        return pltpu.make_async_remote_copy(
            src_ref=where,
            dst_ref=where,
            send_sem=gsend.at[part, index],
            recv_sem=grecv.at[part, index],
            device_id={"tp": to},
            device_id_type=MESH,
        )

    def leaving(part, index):
        owner = (red.me, red.me, red.left, red.me, red.me, red.right)[index]
        low = (0, half, 0, half, 0, half)[index]
        return spread(part, index, owner, low, red.right if index < 3 else red.left)

    def coming(part, index):
        owner = (red.left, red.left, red.far, red.right, red.right, red.far)[index]
        low = (0, half, 0, half, 0, half)[index]
        return spread(part, index, owner, low, red.right if index < 3 else red.left)

    def finish(part):
        red.wait_final(part)

        def body(i, carry):
            at = part * part_rows + i * 16
            here = pl.ds(pl.multiple_of(at, 16), 16)
            after = (residual_ref[here, :].astype(F32) + red.total(here)).astype(BF16)
            after_ref[here, :] = after
            x = after.astype(F32)
            scale = lax.rsqrt(jnp.mean(x * x, axis=1, keepdims=True) + 1e-06)
            x_ref[pl.ds(pl.multiple_of(red.me * rows + at, 16), 16), :] = (
                x * scale * gain_ref[...].astype(F32)
            ).astype(BF16)
            return carry

        lax.fori_loop(0, part_rows // 16, body, 0)
        for n in (0, 3, 1, 4):
            leaving(part, n).start()

    def pass_on(part):
        for n in (0, 3):
            coming(part, n).wait_recv()
            leaving(part, n + 2).start()

    red.combine(0)
    for n in (0, 3, 1, 4):
        red.leg(1, n).start()
    service.run(at + 65, at + 110)
    finish(0)
    service.run(at + 110, at + 170)
    red.combine(1)
    service.run(at + 170, at + 270)
    pass_on(0)
    service.run(at + 270, at + 320)
    finish(1)
    service.run(at + 320, at + 430)
    pass_on(1)
    service.close(at + 430)
    for part in range(ROW_PARTS):
        for n in (1, 2, 4, 5):
            coming(part, n).wait_recv()
        for n in range(6):
            leaving(part, n).wait_send()
    red.wait_sends()


def feed_part(x_ref, weight_ref, after_ref, out_ref, *scratch):
    buffers, (send, recv, hidden) = scratch[:8], scratch[8:]
    red = Reducer("tp", buffers, send, recv)
    blocks, own = buffers[0], buffers[1]
    rows, width = own.shape
    units = weight_ref.shape[1] // 3
    tiles = units // 256

    def make(owner, slot):
        source = pl.ds(pl.multiple_of(owner * rows, 64), rows)

        def inner(j, carry):
            low = pl.multiple_of(j * 256, 256)
            x = x_ref[source, :]
            gate = matmul(x, weight_ref[:, pl.ds(low, 256)])
            up = matmul(x, weight_ref[:, pl.ds(pl.multiple_of(units + low, 256), 256)])
            hidden[:, pl.ds(low, 256)] = (silu_gate(gate) * up).astype(BF16)
            return carry

        lax.fori_loop(0, tiles, inner, 0)

        def body(j, carry):
            columns = pl.ds(pl.multiple_of(j * 256, 256), 256)
            product = matmul(
                hidden[...], weight_ref[columns, 2 * units : 3 * units], ((1,), (1,))
            )
            if slot is None:
                own[:, columns] = product
            else:
                blocks[slot, :, columns] = product.astype(BF16)
            return carry

        lax.fori_loop(0, width // 256, body, 0)

    make(red.far, 0)
    red.leg(0, 0).start()
    red.leg(0, 3).start()
    make(red.right, 1)
    red.leg(0, 1).start()
    make(red.left, 2)
    red.leg(0, 4).start()
    red.combine(0)
    for n in (0, 3, 1, 4):
        red.leg(1, n).start()
    make(red.me, None)

    def finish(part):
        red.wait_final(part)

        def body(i, carry):
            here = pl.ds(pl.multiple_of(part * red.rows + i * 16, 16), 16)
            out_ref[here, :] = (
                after_ref[here, :].astype(F32) + 0.5 * red.total(here)
            ).astype(BF16)
            return carry

        lax.fori_loop(0, red.rows // 16, body, 0)

    finish(0)
    red.combine(1)
    finish(1)
    red.wait_sends()


def greet_all(me, peers, reply):
    core = lax.rem(me, 2)
    chip = me // 2
    last = peers // 2 - 1
    side = lax.axis_index("tp")
    barrier = pltpu.get_barrier_semaphore()

    def hail(axis, other):
        pl.semaphore_signal(barrier, inc=1, device_id={axis: other}, device_id_type=MESH)

    hail("tp", lax.rem(side + 1, 4))
    hail("tp", lax.rem(side + 3, 4))
    hail("sp", me + 1 - 2 * core)

    @pl.when(chip > 0)
    def _():
        hail("sp", me - 1 - core)
        hail("sp", me - 2)

    @pl.when(chip < last)
    def _():
        hail("sp", me + 2)

    below = (chip > 0).astype(jnp.int32)
    above = (chip < last).astype(jnp.int32)
    pl.semaphore_wait(barrier, 3 + below + above + 2 * above * core + 1 - above)

    @pl.when(chip == 0)
    def _():
        hail("sp", me + 2 * last)

    @pl.when(chip == last)
    def _():
        pl.semaphore_signal(
            reply, inc=1, device_id={"sp": me - 2 * last}, device_id_type=MESH
        )


class Gatherer:
    def __init__(self, peers, shards, weights, sems):
        self.me = lax.axis_index("sp")
        self.peers = peers
        self.core = lax.rem(self.me, 2)
        self.chip = self.me // 2
        self.chips = peers // 2
        self.up_steps = self.chips // 2
        self.down_steps = self.chips - 1 - self.up_steps
        self.shards, self.weights = shards, weights
        (self.own_sem, self.up_send, self.up_recv, self.down_send, self.down_recv,
         self.side_send, self.side_recv, self.reply) = sems
        self.depth = shards[0].shape[0]

    def own(self, n):
        units = self.shards[n].shape[1]
        return pltpu.make_async_copy(
            self.shards[n],
            self.weights.at[
                pl.ds(pl.multiple_of(self.me * self.depth, 64), self.depth), pl.ds(n * units, units)
            ],
            self.own_sem.at[n],
        )

    def begin(self):
        for n in range(3):
            self.own(n).start()

    def move(self, chip, core, to, send, recv):
        place = self.weights.at[
            pl.ds(pl.multiple_of((2 * chip + core) * self.depth, 64), self.depth)
        ]
        return pltpu.make_async_remote_copy(
            src_ref=place,
            dst_ref=place,
            send_sem=send,
            recv_sem=recv,
            device_id={"sp": to},
            device_id_type=MESH,
        )

    def up(self, k, distance=None):
        origin = lax.rem(self.chip + self.chips - (k if distance is None else distance), self.chips)
        to = lax.rem(self.me + 2, self.peers)
        return self.move(origin, self.core, to, self.up_send.at[k], self.up_recv.at[k])

    def down(self, k, distance=None):
        origin = lax.rem(self.chip + (k if distance is None else distance), self.chips)
        to = lax.rem(self.me + self.peers - 2, self.peers)
        return self.move(origin, self.core, to, self.down_send.at[k], self.down_recv.at[k])

    def side(self, chip, core):
        to = self.me + 1 - 2 * self.core
        return self.move(chip, core, to, self.side_send.at[chip], self.side_recv.at[chip])

    def open(self):
        for n in range(3):
            self.own(n).wait()
        self.up(0).start()

        @pl.when(self.chip > 0)
        def _():
            self.down(0).start()

        self.side(self.chip, self.core).start()

    def open_last(self):
        @pl.when(self.chip == 0)
        def _():
            pl.semaphore_wait(self.reply, 1)
            self.down(0).start()

    def due(self, at):
        near = jnp.maximum((at - 70) // 60, 0)
        wrapped = (at - 294) // 60
        up = jnp.minimum(
            jnp.where(wrapped > self.chip, wrapped, jnp.minimum(near, self.chip)), self.up_steps
        )
        near = jnp.maximum((at - 70) // 88, 0)
        wrapped = (at + 154) // 88
        down = jnp.minimum(
            jnp.where(near <= self.chips - 1 - self.chip, near, wrapped), self.down_steps
        )
        down = jnp.where((self.chip == 0) & (at < 275), 0, down)
        return up, down

    def steps(self, first, then):
        def step_up(i, carry):
            self.up(i, i + 1).wait_recv()

            @pl.when(i + 1 < self.up_steps)
            def _():
                self.up(i + 1).start()

            self.side(lax.rem(self.chip + self.chips - i - 1, self.chips), self.core).start()
            return carry

        def step_down(i, carry):
            self.down(i, i + 1).wait_recv()

            @pl.when(i + 1 < self.down_steps)
            def _():
                self.down(i + 1).start()

            self.side(lax.rem(self.chip + i + 1, self.chips), self.core).start()
            return carry

        lax.fori_loop(first[0], then[0], step_up, 0)
        lax.fori_loop(first[1], then[1], step_down, 0)

    def run(self, at, until):
        self.steps(self.due(at), self.due(until))

    def close(self, at):
        self.steps(self.due(at), (self.up_steps, self.down_steps))

        def arrive(i, carry):
            self.side(i, 1 - self.core).wait_recv()
            return carry

        lax.fori_loop(0, self.chips, arrive, 0)

    def drain(self):
        def up(i, carry):
            self.up(i).wait_send()
            return carry

        def down(i, carry):
            self.down(i).wait_send()
            return carry

        def side(i, carry):
            self.side(i, self.core).wait_send()
            return carry

        lax.fori_loop(0, self.up_steps, up, 0)
        lax.fori_loop(0, self.down_steps, down, 0)
        lax.fori_loop(0, self.chips, side, 0)


def layer_kernel(peers, counts, *refs):
    refs = list(refs)

    def take(n):
        out = refs[:n]
        del refs[:n]
        return out

    mixer_in = take(15)
    output_ref, residual_ref, norm_gain_ref = take(3)
    shards = take(3)
    (out_ref,) = take(1)
    (normed,) = take(1)
    mixer_scratch = take(counts[0])
    weight, residual, x, after, load_sem = take(5)
    project_scratch = take(12)
    feed_scratch = take(11)
    (weights,) = take(1)
    sems = take(8)
    service = Gatherer(peers, shards, weights, sems)
    service.begin()
    loads = (
        pltpu.make_async_copy(output_ref, weight, load_sem.at[0]),
        pltpu.make_async_copy(residual_ref, residual, load_sem.at[1]),
    )
    for load in loads:
        load.start()
    at = mixer_part(peers, service, *mixer_in, normed, *mixer_scratch)
    for load in loads:
        load.wait()
    project_part(
        service, at, normed, weight, residual, norm_gain_ref, x, after, *project_scratch
    )
    feed_part(x, weights, after, out_ref, *feed_scratch)
    service.drain()


def layer(arrays, output_matrix, residual, norm_gain, shards, peers):
    length = arrays[0].shape[0]
    channels = arrays[0].shape[1]
    rows, width = residual.shape
    span = sum(a.shape[1] for a in arrays[:5])
    depth, units = shards[0].shape
    count = length // CH
    hbm = pl.BlockSpec(memory_space=pltpu.HBM)
    vmem = pl.BlockSpec(memory_space=pltpu.VMEM)
    dma = pltpu.SemaphoreType.DMA
    chips = peers // 2
    mixer_scratch = [
        pltpu.VMEM((PAD + length, span), BF16),
        pltpu.VMEM((length, channels), BF16),
        pltpu.VMEM((length, 384), BF16),
        pltpu.VMEM((length, 512), BF16),
        pltpu.VMEM((length, channels), BF16),
        pltpu.VMEM((length, 16), F32),
        pltpu.VMEM((count, 16, CH), F32),
        pltpu.VMEM((count, 1, 16), F32),
        pltpu.VMEM((count, 384, 256), F32),
        pltpu.VMEM((count, 384, 256), BF16),
        pltpu.VMEM((length, channels), F32),
        pltpu.VMEM((384, 256), F32),
        pltpu.VMEM((384, 256), BF16),
        pltpu.VMEM((400, 256), BF16),
        pltpu.VMEM((400, 256), BF16),
        pltpu.VMEM((384, 256), BF16),
        pltpu.VMEM((384, 256), BF16),
        dma((6,)),
        dma((5,)),
        dma((5,)),
        dma((2,)),
        dma((2,)),
        dma((384 // PIECE,)),
        dma((384 // PIECE,)),
    ]
    scratch = (
        [pltpu.VMEM((length, channels), BF16)]
        + mixer_scratch
        + [
            pltpu.VMEM(output_matrix.shape, BF16),
            pltpu.VMEM((rows, width), BF16),
            pltpu.VMEM((4 * rows, width), BF16),
            pltpu.VMEM((rows, width), BF16),
            dma((2,)),
        ]
        + reducer_scratch(rows, width)
        + [dma((ROW_PARTS, 6)), dma((ROW_PARTS, 6))]
        + reducer_scratch(rows, width)
        + [pltpu.VMEM((rows, units), BF16)]
        + [pltpu.VMEM((peers * depth, 3 * units), BF16)]
        + [
            dma((3,)),
            dma((chips,)),
            dma((chips,)),
            dma((chips,)),
            dma((chips,)),
            dma((chips,)),
            dma((chips,)),
            pltpu.SemaphoreType.REGULAR,
        ]
    )
    return pl.pallas_call(
        functools.partial(layer_kernel, peers, (len(mixer_scratch),)),
        out_shape=jax.ShapeDtypeStruct((rows, width), BF16),
        in_specs=[hbm] * 6 + [vmem] * 9 + [hbm, hbm, vmem] + [hbm] * 3,
        out_specs=vmem,
        scratch_shapes=scratch,
        compiler_params=pltpu.CompilerParams(
            collective_id=1, has_side_effects=True, vmem_limit_bytes=62 * 1024 * 1024
        ),
        cost_estimate=pl.CostEstimate(
            flops=40_000_000_000, bytes_accessed=20_000_000, transcendentals=0
        ),
        name="layer",
    )(*arrays, output_matrix, residual, norm_gain, *shards)


def on_device(
    residual,
    value_projected,
    gate_projected,
    wide_key_rows,
    wide_query_rows,
    narrow_key_rows,
    narrow_query_rows,
    step_before_softplus,
    extra_log_decay,
    log_decay_rate,
    value_kernel,
    wide_key_kernel,
    wide_query_kernel,
    narrow_key_kernel,
    narrow_query_kernel,
    head_norm_gain,
    output_matrix,
    feedforward_norm_gain,
    gate_matrix,
    up_matrix,
    down_matrix,
):
    return layer(
        [
            value_projected,
            wide_key_rows,
            wide_query_rows,
            narrow_key_rows,
            narrow_query_rows,
            gate_projected,
            step_before_softplus.T,
            extra_log_decay.T,
            log_decay_rate[None],
            value_kernel,
            wide_key_kernel,
            wide_query_kernel,
            narrow_key_kernel,
            narrow_query_kernel,
            head_norm_gain[None],
        ],
        output_matrix,
        residual,
        feedforward_norm_gain[None],
        (gate_matrix, up_matrix, down_matrix),
        lax.axis_size("sp"),
    )


def solution(mesh):
    in_specs = (
        P(("grp", "sp", "tp"), None),
        P(("grp", "sp"), "tp"),
        P(("grp", "sp"), "tp"),
        P(("grp", "sp"), "tp"),
        P(("grp", "sp"), "tp"),
        P(("grp", "sp"), "tp"),
        P(("grp", "sp"), "tp"),
        P(("grp", "sp"), "tp"),
        P(("grp", "sp"), "tp"),
        P("tp"),
        P(None, "tp"),
        P(None, "tp"),
        P(None, "tp"),
        P(None, "tp"),
        P(None, "tp"),
        P("tp"),
        P("tp", None),
        P(),
        P("sp", "tp"),
        P("sp", "tp"),
        P("sp", "tp"),
    )
    out_specs = P(("grp", "sp", "tp"), None)
    return jax.shard_map(
        on_device, mesh=mesh, in_specs=in_specs, out_specs=out_specs, check_vma=False
    )
```

```python
import functools
import jax
import jax.numpy as jnp
from jax import lax
from jax.experimental import pallas as pl
from jax.experimental.pallas import tpu as pltpu
from jax.sharding import PartitionSpec as P

F32 = jnp.float32
BF16 = jnp.bfloat16
MESH = pl.DeviceIdType.MESH
CH = 128
PAD = 16
PIECE = 16
GROUP_Q = (0, 256, 128, 384)
GROUP_K = (0, 256, 128, 256)
ROW_GROUP = ((0, 128, 0), (128, 256, 2), (256, 320, 1), (320, 384, 3))
HIGH = lax.Precision.HIGHEST


def pair_lanes(columns, head):
    rows = columns.shape[0]
    lane = lax.broadcasted_iota(jnp.int32, (rows, 128), 1)
    return jnp.where(
        lane < 64,
        jnp.broadcast_to(columns[:, head : head + 1], (rows, 128)),
        jnp.broadcast_to(columns[:, head + 1 : head + 2], (rows, 128)),
    )


def quad_lanes(columns, group):
    return jnp.concatenate(
        [pair_lanes(columns, 4 * group), pair_lanes(columns, 4 * group + 2)], axis=1
    )


def silu(x):
    return x / (1.0 + jnp.exp(-x))


def matmul(a, b, dims=((1,), (0,)), precision=None):
    return lax.dot_general(a, b, (dims, ((), ())), preferred_element_type=F32, precision=precision)


def group_of_row(row):
    for low, high, group in ROW_GROUP:
        if low <= row < high:
            return group


def mixer_part(
    peers,
    service,
    value_ref,
    wk_ref,
    wq_ref,
    nk_ref,
    nq_ref,
    gate_ref,
    step_ref,
    extra_ref,
    rate_ref,
    vker_ref,
    wkker_ref,
    wqker_ref,
    nkker_ref,
    nqker_ref,
    gain_ref,
    normed_ref,
    xpad,
    ubuf,
    kbuf,
    qbuf,
    gbuf,
    rcol,
    qrow,
    total,
    ebuf,
    hbuf,
    ybuf,
    hent,
    entered_ref,
    half_out,
    half_in,
    chain_in,
    chain_out,
    local_sem,
    rim_send,
    rim_recv,
    swap_send,
    swap_recv,
    chain_send,
    chain_recv,
):
    length = value_ref.shape[0]
    count = length // CH
    me = lax.axis_index("sp")
    inputs = (value_ref, wk_ref, wq_ref, nk_ref, nq_ref)
    spans = []
    at = 0
    for ref in inputs:
        spans.append((at, at + ref.shape[1]))
        at += ref.shape[1]
    loads = [
        pltpu.make_async_copy(
            ref, xpad.at[pl.ds(PAD, length), pl.ds(low, high - low)], local_sem.at[n]
        )
        for n, (ref, (low, high)) in enumerate(zip(inputs, spans))
    ]
    loads.append(pltpu.make_async_copy(gate_ref, gbuf, local_sem.at[len(inputs)]))
    for load in loads:
        load.start()
    core = lax.rem(me, 2)
    chip = me // 2
    chips = peers // 2
    partner = me + 1 - 2 * core

    def send_to(peer, source, target, send, recv):
        return pltpu.make_async_remote_copy(
            src_ref=source,
            dst_ref=target,
            send_sem=send,
            recv_sem=recv,
            device_id={"sp": peer},
            device_id_type=MESH,
        )

    def rim(n):
        low, high = spans[n]
        return send_to(
            lax.rem(me + 1, peers),
            inputs[n].at[pl.ds(length - PAD, PAD)],
            xpad.at[pl.ds(0, PAD), pl.ds(low, high - low)],
            rim_send.at[n],
            rim_recv.at[n],
        )

    greet_all(me, peers, service.reply)
    service.open()

    @pl.when(me < peers - 1)
    def _():
        for n in range(len(inputs)):
            rim(n).start()

    for load in loads[:-1]:
        load.wait()

    row_id = lax.broadcasted_iota(jnp.int32, (CH, CH), 0)
    col_id = lax.broadcasted_iota(jnp.int32, (CH, CH), 1)
    lower = row_id >= col_id
    tril = lower.astype(F32)
    triu = (row_id <= col_id).astype(F32)
    eye = (row_id == col_id).astype(F32)
    left = lax.broadcasted_iota(jnp.int32, (CH, 128), 1) < 64
    diagonal = lax.broadcasted_iota(jnp.int32, (16, 16), 0) == lax.broadcasted_iota(
        jnp.int32, (16, 16), 1
    )
    rate = -jnp.sum(
        jnp.where(diagonal, jnp.broadcast_to(jnp.exp(rate_ref[...]), (16, 16)), 0.0),
        axis=1,
        keepdims=True,
    )
    kernels = (vker_ref, wkker_ref, wqker_ref, nkker_ref, nqker_ref)

    def conv_tile(base, which, tile):
        low = spans[which][0] + 128 * tile
        columns = pl.ds(low, 128)
        before = xpad[pl.ds(base, PAD), columns].astype(F32)[PAD - 8 :]
        here = xpad[pl.ds(base + PAD, CH), columns].astype(F32)
        rows = jnp.concatenate([before, here], axis=0)
        taps = kernels[which][:, 128 * tile : 128 * tile + 128].astype(F32)
        acc = here * taps[3:4]
        for tap in range(3):
            acc = acc + pltpu.roll(rows, 3 - tap, 0)[8:] * taps[tap : tap + 1]
        return silu(acc)

    def first_pass(i, carry):
        c = lax.rem(i + 1, count)
        base = pl.multiple_of(c * CH, CH)

        @pl.when(i == count - 1)
        def _():
            @pl.when(me > 0)
            def _():
                for n in range(len(inputs)):
                    rim(n).wait_recv()

            @pl.when(me == 0)
            def _():
                xpad[0:PAD, :] = jnp.zeros((PAD, xpad.shape[1]), BF16)

        here = pl.ds(base, CH)
        dt_row = step_ref[:, here]
        dt_row = jnp.maximum(dt_row, 0.0) + jnp.log(1.0 + jnp.exp(-jnp.abs(dt_row)))
        a = rate * dt_row + extra_ref[:, here]
        r = matmul(tril, a, ((1,), (1,)), HIGH)
        r_row = matmul(a, triu, precision=HIGH)
        dt = matmul(eye, dt_row, ((1,), (1,)), HIGH)
        rcol[here, :] = r
        qrow[c] = r_row - jnp.log(dt_row)
        end = r[CH - 1 : CH, :]
        total[c] = end
        fade = dt * jnp.exp(end - r)
        for tile in range(2):
            kbuf[here, 128 * tile : 128 * tile + 128] = conv_tile(base, 1, tile).astype(BF16)
            qbuf[here, 128 * tile : 128 * tile + 128] = conv_tile(base, 2, tile).astype(BF16)
        kbuf[here, 256:384] = conv_tile(base, 3, 0).astype(BF16)
        narrow_q = conv_tile(base, 4, 0)
        qbuf[here, 256:384] = jnp.where(left, narrow_q, 0.0).astype(BF16)
        qbuf[here, 384:512] = jnp.where(left, 0.0, narrow_q).astype(BF16)
        for group in range(4):
            parts = []
            for half in range(2):
                pair = 2 * group + half
                u = conv_tile(base, 0, pair).astype(BF16)
                ubuf[here, 128 * pair : 128 * pair + 128] = u
                parts.append((u.astype(F32) * pair_lanes(fade, 2 * pair)).astype(BF16))
            v = jnp.concatenate(parts, axis=1)
            k = kbuf[here, GROUP_K[group] : GROUP_K[group] + 128]
            e = matmul(k, v, ((0,), (0,)))
            if group == 0:
                ebuf[c, 0:128, :] = e
            elif group == 2:
                ebuf[c, 128:256, :] = e
            elif group == 1:
                ebuf[c, 256:320, :] = e[0:64]
            else:
                ebuf[c, 320:384, :] = e[64:128]
        service.run(20 + 14 * i, 34 + 14 * i)
        return carry

    lax.fori_loop(0, count, first_pass, 0)

    offsets = [jnp.zeros((1, 16), F32)]
    for c in range(count):
        offsets.append(offsets[-1] + total[c])
    whole = offsets[-1]
    for low, high, group in ROW_GROUP:
        state = jnp.zeros((high - low, 256), F32)
        for c in range(count):
            hbuf[c, low:high, :] = state.astype(BF16)
            state = state * jnp.exp(quad_lanes(total[c], group)) + ebuf[c, low:high, :]
        hent[low:high, :] = state

    log_total = [quad_lanes(whole, group) for group in range(4)]
    sub = lax.broadcasted_iota(jnp.int32, (16, 256), 0)
    swap = send_to(partner, half_out, half_in, swap_send.at[0], swap_recv.at[0])

    @pl.when(core == 0)
    def _():
        half_out[0:384, :] = hent[...].astype(BF16)
        lines = jnp.zeros((16, 256), F32)
        for group in range(4):
            lines = jnp.where(
                sub == group, jnp.broadcast_to(log_total[group], (16, 256)), lines
            )
        half_out[384:400, :] = lines.astype(BF16)
        swap.start()

    def second_pass(c, start):
        here = pl.ds(pl.multiple_of(c * CH, CH), CH)
        r = rcol[here, :]
        fade_out = jnp.exp(r)
        for group in range(4):
            q = qbuf[here, GROUP_Q[group] : GROUP_Q[group] + 128]
            k = kbuf[here, GROUP_K[group] : GROUP_K[group] + 128]
            score = matmul(q, k, ((1,), (1,)))
            row = 0 if group == 0 else 128 if group == 2 else 256
            outer = matmul(q, hbuf[c, row : row + 128, :])
            for half in range(2):
                pair = 2 * group + half
                weights = []
                for head in (2 * pair, 2 * pair + 1):
                    gap = jnp.broadcast_to(r[:, head : head + 1], (CH, CH)) - qrow[c, head : head + 1, :]
                    w = score * jnp.exp(jnp.where(lower, gap, -jnp.inf))
                    weights.append(w.astype(BF16))
                u = ubuf[here, 128 * pair : 128 * pair + 128].astype(F32)
                both = jnp.concatenate(
                    [jnp.where(left, u, 0.0).astype(BF16), jnp.where(left, 0.0, u).astype(BF16)],
                    axis=0,
                )
                inner = matmul(jnp.concatenate(weights, axis=1), both)
                ybuf[here, 128 * pair : 128 * pair + 128] = (
                    inner + outer[:, 128 * half : 128 * half + 128] * pair_lanes(fade_out, 2 * pair)
                )
        service.run(start + 11 * c, start + 11 * c + 11)
        return start

    early = jnp.minimum(count, 1 + chip // 2)
    service.run(20 + 14 * count, 120)
    lax.fori_loop(0, early, second_pass, 120)

    def link(piece):
        rows = pl.ds(piece * PIECE, PIECE)
        return send_to(
            lax.rem(me + 2, peers),
            chain_out.at[rows],
            chain_in.at[rows],
            chain_send.at[piece],
            chain_recv.at[piece],
        )

    hand = send_to(partner, chain_in, entered_ref, swap_send.at[1], swap_recv.at[1])

    @pl.when(core == 1)
    def _():
        swap.wait_recv()
        lines = half_in[384:400, :].astype(F32)
        fade_0 = [jnp.exp(lines[group : group + 1]) for group in range(4)]
        fade_1 = [jnp.exp(line) for line in log_total]

        @pl.when(chip == 0)
        def _():
            chain_in[...] = jnp.zeros_like(chain_in)

        for piece in range(384 // PIECE):

            @pl.when(chip > 0)
            def _():
                link(piece).wait_recv()

            for at in range(piece * PIECE, piece * PIECE + PIECE, 16):
                group = group_of_row(at)
                rows = slice(at, at + 16)
                second = (
                    chain_in[rows, :].astype(F32) * fade_0[group] + half_in[rows, :].astype(F32)
                )
                chain_out[rows, :] = (second * fade_1[group] + hent[rows, :]).astype(BF16)
                entered_ref[rows, :] = second.astype(BF16)

            @pl.when(chip < chips - 1)
            def _():
                link(piece).start()

        hand.start()

    service.run(120 + 11 * early, 130 + 6 * chip)
    lax.fori_loop(early, count, second_pass, 130 + 6 * chip - 11 * early)
    at = 130 + 6 * chip + 11 * (count - early)
    loads[-1].wait()

    @pl.when(core == 0)
    def _():
        swap.wait_send()
        hand.wait_recv()

    @pl.when(core == 1)
    def _():
        hand.wait_send()

    @pl.when((chip < chips - 1) & (core == 1))
    def _():
        for piece in range(384 // PIECE):
            link(piece).wait_send()

    @pl.when(me < peers - 1)
    def _():
        for n in range(len(inputs)):
            rim(n).wait_send()

    ones = (
        (row_id < 64) == (col_id < 64)
    ).astype(BF16)

    for c in range(count):
        here = slice(c * CH, c * CH + CH)
        reach = jnp.exp(rcol[here, :] + offsets[c])
        for group in range(4):
            q = qbuf[here, GROUP_Q[group] : GROUP_Q[group] + 128]
            row = 0 if group == 0 else 128 if group == 2 else 256
            entered = matmul(q, entered_ref[row : row + 128, :])
            for half in range(2):
                pair = 2 * group + half
                lanes = slice(128 * pair, 128 * pair + 128)
                y = ybuf[here, lanes]
                y = y + entered[:, 128 * half : 128 * half + 128] * pair_lanes(reach, 2 * pair)
                gated = y * silu(gbuf[here, lanes].astype(F32))
                square = matmul((gated * gated).astype(BF16), ones)
                scale = lax.rsqrt(square * (1.0 / 64.0) + 1e-06)
                normed_ref[here, lanes] = (
                    gated * scale * gain_ref[:, lanes].astype(F32)
                ).astype(BF16)
        service.run(at, at + 6)
        at = at + 6
    return at


ROW_PARTS = 2


def silu_gate(x):
    return x / (1.0 + jnp.exp(-x))


class Reducer:
    def __init__(self, axis, buffers, send, recv):
        self.me = lax.axis_index(axis)
        self.right = lax.rem(self.me + 1, 4)
        self.left = lax.rem(self.me + 3, 4)
        self.far = lax.rem(self.me + 2, 4)
        self.axis = axis
        (self.blocks, self.own, self.relay_r, self.relay_l, self.comb_r, self.comb_l,
         self.from_l, self.from_r) = buffers
        self.send, self.recv = send, recv
        self.rows = self.own.shape[0] // ROW_PARTS
        self.half = self.own.shape[1] // 2

    def copy(self, part, index, source, target, to):
        return pltpu.make_async_remote_copy(
            src_ref=source,
            dst_ref=target,
            send_sem=self.send.at[part, index],
            recv_sem=self.recv.at[part, index],
            device_id={self.axis: to},
            device_id_type=MESH,
        )

    def leg(self, part, index):
        rows = pl.ds(part * self.rows, self.rows)
        a, b = pl.ds(0, self.half), pl.ds(self.half, self.half)
        source, target = (
            (self.blocks.at[0, rows, a], self.relay_r.at[rows]),
            (self.blocks.at[1, rows, b], self.from_l.at[rows, b]),
            (self.comb_r.at[rows], self.from_l.at[rows, a]),
            (self.blocks.at[0, rows, b], self.relay_l.at[rows]),
            (self.blocks.at[2, rows, a], self.from_r.at[rows, a]),
            (self.comb_l.at[rows], self.from_r.at[rows, b]),
        )[index]
        return self.copy(part, index, source, target, self.right if index < 3 else self.left)

    def combine(self, part):
        step = 32

        for n, block, low, relay, comb in (
            (0, 1, 0, self.relay_r, self.comb_r),
            (3, 2, self.half, self.relay_l, self.comb_l),
        ):
            self.leg(part, n).wait_recv()

            def body(i, carry, block=block, low=low, relay=relay, comb=comb):
                rows = pl.ds(pl.multiple_of(part * self.rows + i * step, 16), step)
                comb[rows, :] = (
                    self.blocks[block, rows, low : low + self.half].astype(F32)
                    + relay[rows, :].astype(F32)
                ).astype(BF16)
                return carry

            lax.fori_loop(0, self.rows // step, body, 0)
            self.leg(part, n + 2).start()

    def wait_final(self, part):
        for n in (1, 2, 4, 5):
            self.leg(part, n).wait_recv()

    def wait_sends(self):
        for part in range(ROW_PARTS):
            for n in range(6):
                self.leg(part, n).wait_send()

    def total(self, rows):
        return (
            self.own[rows, :]
            + self.from_l[rows, :].astype(F32)
            + self.from_r[rows, :].astype(F32)
        )


def reducer_scratch(rows, width):
    half = width // 2
    dma = pltpu.SemaphoreType.DMA
    return [
        pltpu.VMEM((3, rows, width), BF16),
        pltpu.VMEM((rows, width), F32),
        pltpu.VMEM((rows, half), BF16),
        pltpu.VMEM((rows, half), BF16),
        pltpu.VMEM((rows, half), BF16),
        pltpu.VMEM((rows, half), BF16),
        pltpu.VMEM((rows, width), BF16),
        pltpu.VMEM((rows, width), BF16),
        dma((ROW_PARTS, 6)),
        dma((ROW_PARTS, 6)),
    ]


def project_part(
    service, at, normed_ref, weight_ref, residual_ref, gain_ref, x_ref, after_ref, *scratch
):
    buffers, (send, recv, gsend, grecv) = scratch[:8], scratch[8:]
    red = Reducer("tp", buffers, send, recv)
    blocks, own = buffers[0], buffers[1]
    rows, width = own.shape
    half = width // 2

    def make(owner, slot):
        source = pl.ds(pl.multiple_of(owner * rows, 64), rows)

        def body(j, carry):
            columns = pl.ds(pl.multiple_of(j * 256, 256), 256)
            product = matmul(normed_ref[source, :], weight_ref[:, columns])
            if slot is None:
                own[:, columns] = product
            else:
                blocks[slot, :, columns] = product.astype(BF16)
            return carry

        lax.fori_loop(0, width // 256, body, 0)

    make(red.far, 0)
    red.leg(0, 0).start()
    red.leg(0, 3).start()
    service.run(at, at + 14)
    make(red.right, 1)
    red.leg(0, 1).start()
    service.run(at + 14, at + 28)
    make(red.left, 2)
    red.leg(0, 4).start()
    service.run(at + 28, at + 42)
    make(red.me, None)
    service.open_last()
    service.run(at + 42, at + 65)

    part_rows = red.rows

    def spread(part, index, owner, low, to):
        where = x_ref.at[
            pl.ds(pl.multiple_of(owner * rows + part * part_rows, 32), part_rows),
            pl.ds(low, half),
        ]
        return pltpu.make_async_remote_copy(
            src_ref=where,
            dst_ref=where,
            send_sem=gsend.at[part, index],
            recv_sem=grecv.at[part, index],
            device_id={"tp": to},
            device_id_type=MESH,
        )

    def leaving(part, index):
        owner = (red.me, red.me, red.left, red.me, red.me, red.right)[index]
        low = (0, half, 0, half, 0, half)[index]
        return spread(part, index, owner, low, red.right if index < 3 else red.left)

    def coming(part, index):
        owner = (red.left, red.left, red.far, red.right, red.right, red.far)[index]
        low = (0, half, 0, half, 0, half)[index]
        return spread(part, index, owner, low, red.right if index < 3 else red.left)

    def finish(part):
        red.wait_final(part)

        def body(i, carry):
            at = part * part_rows + i * 16
            here = pl.ds(pl.multiple_of(at, 16), 16)
            after = (residual_ref[here, :].astype(F32) + red.total(here)).astype(BF16)
            after_ref[here, :] = after
            x = after.astype(F32)
            scale = lax.rsqrt(jnp.mean(x * x, axis=1, keepdims=True) + 1e-06)
            x_ref[pl.ds(pl.multiple_of(red.me * rows + at, 16), 16), :] = (
                x * scale * gain_ref[...].astype(F32)
            ).astype(BF16)
            return carry

        lax.fori_loop(0, part_rows // 16, body, 0)
        for n in (0, 3, 1, 4):
            leaving(part, n).start()

    def pass_on(part):
        for n in (0, 3):
            coming(part, n).wait_recv()
            leaving(part, n + 2).start()

    red.combine(0)
    for n in (0, 3, 1, 4):
        red.leg(1, n).start()
    service.run(at + 65, at + 110)
    finish(0)
    service.run(at + 110, at + 170)
    red.combine(1)
    service.run(at + 170, at + 270)
    pass_on(0)
    service.run(at + 270, at + 320)
    finish(1)
    service.run(at + 320, at + 430)
    pass_on(1)
    service.close(at + 430)
    for part in range(ROW_PARTS):
        for n in (1, 2, 4, 5):
            coming(part, n).wait_recv()
        for n in range(6):
            leaving(part, n).wait_send()
    red.wait_sends()


def feed_part(x_ref, weight_ref, after_ref, out_ref, *scratch):
    buffers, (send, recv, hidden) = scratch[:8], scratch[8:]
    red = Reducer("tp", buffers, send, recv)
    blocks, own = buffers[0], buffers[1]
    rows, width = own.shape
    units = weight_ref.shape[1] // 3
    tiles = units // 256

    def make(owner, slot):
        source = pl.ds(pl.multiple_of(owner * rows, 64), rows)

        def inner(j, carry):
            low = pl.multiple_of(j * 256, 256)
            x = x_ref[source, :]
            gate = matmul(x, weight_ref[:, pl.ds(low, 256)])
            up = matmul(x, weight_ref[:, pl.ds(pl.multiple_of(units + low, 256), 256)])
            hidden[:, pl.ds(low, 256)] = (silu_gate(gate) * up).astype(BF16)
            return carry

        lax.fori_loop(0, tiles, inner, 0)

        def body(j, carry):
            columns = pl.ds(pl.multiple_of(j * 256, 256), 256)
            product = matmul(
                hidden[...], weight_ref[columns, 2 * units : 3 * units], ((1,), (1,))
            )
            if slot is None:
                own[:, columns] = product
            else:
                blocks[slot, :, columns] = product.astype(BF16)
            return carry

        lax.fori_loop(0, width // 256, body, 0)

    make(red.far, 0)
    red.leg(0, 0).start()
    red.leg(0, 3).start()
    make(red.right, 1)
    red.leg(0, 1).start()
    make(red.left, 2)
    red.leg(0, 4).start()
    red.combine(0)
    for n in (0, 3, 1, 4):
        red.leg(1, n).start()
    make(red.me, None)

    def finish(part):
        red.wait_final(part)

        def body(i, carry):
            here = pl.ds(pl.multiple_of(part * red.rows + i * 16, 16), 16)
            out_ref[here, :] = (
                after_ref[here, :].astype(F32) + 0.5 * red.total(here)
            ).astype(BF16)
            return carry

        lax.fori_loop(0, red.rows // 16, body, 0)

    finish(0)
    red.combine(1)
    finish(1)
    red.wait_sends()


def greet_all(me, peers, reply):
    core = lax.rem(me, 2)
    chip = me // 2
    last = peers // 2 - 1
    side = lax.axis_index("tp")
    barrier = pltpu.get_barrier_semaphore()

    def hail(axis, other):
        pl.semaphore_signal(barrier, inc=1, device_id={axis: other}, device_id_type=MESH)

    hail("tp", lax.rem(side + 1, 4))
    hail("tp", lax.rem(side + 3, 4))
    hail("sp", me + 1 - 2 * core)

    @pl.when(chip > 0)
    def _():
        hail("sp", me - 1 - core)
        hail("sp", me - 2)

    @pl.when(chip < last)
    def _():
        hail("sp", me + 2)

    below = (chip > 0).astype(jnp.int32)
    above = (chip < last).astype(jnp.int32)
    pl.semaphore_wait(barrier, 3 + below + above + 2 * above * core + 1 - above)

    @pl.when(chip == 0)
    def _():
        hail("sp", me + 2 * last)

    @pl.when(chip == last)
    def _():
        pl.semaphore_signal(
            reply, inc=1, device_id={"sp": me - 2 * last}, device_id_type=MESH
        )


PARTS = 3


class Gatherer:
    def __init__(self, peers, shards, weights, sems):
        self.me = lax.axis_index("sp")
        self.peers = peers
        self.core = lax.rem(self.me, 2)
        self.chip = self.me // 2
        self.chips = peers // 2
        self.up_steps = PARTS * (self.chips // 2)
        self.down_steps = PARTS * (self.chips - 1) - self.up_steps
        self.shards, self.weights = shards, weights
        (self.own_sem, self.up_send, self.up_recv, self.down_send, self.down_recv,
         self.side_send, self.side_recv, self.reply) = sems
        self.depth = shards[0].shape[0]

    def own(self, n):
        return pltpu.make_async_copy(
            self.shards[n], self.place(self.chip, self.core, n), self.own_sem.at[n]
        )

    def place(self, chip, core, part):
        units = self.shards[0].shape[1]
        return self.weights.at[
            pl.ds(pl.multiple_of((2 * chip + core) * self.depth, 64), self.depth),
            pl.ds(pl.multiple_of(part * units, 128), units),
        ]

    def begin(self):
        for n in range(3):
            self.own(n).start()

    def move(self, place, to, send, recv):
        return pltpu.make_async_remote_copy(
            src_ref=place,
            dst_ref=place,
            send_sem=send,
            recv_sem=recv,
            device_id={"sp": to},
            device_id_type=MESH,
        )

    def up(self, k, hops=0):
        distance = k // PARTS + hops
        origin = lax.rem(self.chip + self.chips - distance, self.chips)
        to = lax.rem(self.me + 2, self.peers)
        place = self.place(origin, self.core, lax.rem(k, PARTS))
        return self.move(place, to, self.up_send.at[k], self.up_recv.at[k])

    def down(self, k, hops=0):
        distance = k // PARTS + hops
        origin = lax.rem(self.chip + distance, self.chips)
        to = lax.rem(self.me + self.peers - 2, self.peers)
        place = self.place(origin, self.core, lax.rem(k, PARTS))
        return self.move(place, to, self.down_send.at[k], self.down_recv.at[k])

    def side(self, k, core):
        to = self.me + 1 - 2 * self.core
        place = self.place(k // PARTS, core, lax.rem(k, PARTS))
        return self.move(place, to, self.side_send.at[k], self.side_recv.at[k])

    def open(self):
        for n in range(PARTS):
            self.own(n).wait()
            self.up(n).start()

            @pl.when(self.chip > 0)
            def _():
                self.down(n).start()

            self.side(self.chip * PARTS + n, self.core).start()

    def open_last(self):
        @pl.when(self.chip == 0)
        def _():
            pl.semaphore_wait(self.reply, 1)
            for n in range(PARTS):
                self.down(n).start()

    def due(self, at):
        near = jnp.maximum((at - 55) // 20, 0)
        wrapped = (at - 279) // 20
        limit = PARTS * self.chip
        up = jnp.minimum(
            jnp.where(wrapped > limit, wrapped, jnp.minimum(near, limit)), self.up_steps
        )
        down = jnp.minimum(jnp.maximum((at - 90) // 27, 0), self.down_steps)
        down = jnp.where((self.chip == 0) & (at < 275), 0, down)
        return up, down

    def steps(self, first, then):
        def step_up(i, carry):
            self.up(i, 1).wait_recv()

            @pl.when(i + PARTS < self.up_steps)
            def _():
                self.up(i + PARTS).start()

            origin = lax.rem(self.chip + self.chips - i // PARTS - 1, self.chips)
            self.side(origin * PARTS + lax.rem(i, PARTS), self.core).start()
            return carry

        def step_down(i, carry):
            self.down(i, 1).wait_recv()

            @pl.when(i + PARTS < self.down_steps)
            def _():
                self.down(i + PARTS).start()

            origin = lax.rem(self.chip + i // PARTS + 1, self.chips)
            self.side(origin * PARTS + lax.rem(i, PARTS), self.core).start()
            return carry

        lax.fori_loop(first[0], then[0], step_up, 0)
        lax.fori_loop(first[1], then[1], step_down, 0)

    def run(self, at, until):
        self.steps(self.due(at), self.due(until))

    def close(self, at):
        self.steps(self.due(at), (self.up_steps, self.down_steps))

        def arrive(i, carry):
            self.side(i, 1 - self.core).wait_recv()
            return carry

        lax.fori_loop(0, PARTS * self.chips, arrive, 0)

    def drain(self):
        def up(i, carry):
            self.up(i).wait_send()
            return carry

        def down(i, carry):
            self.down(i).wait_send()
            return carry

        def side(i, carry):
            self.side(i, self.core).wait_send()
            return carry

        lax.fori_loop(0, self.up_steps, up, 0)
        lax.fori_loop(0, self.down_steps, down, 0)
        lax.fori_loop(0, PARTS * self.chips, side, 0)


def layer_kernel(peers, counts, *refs):
    refs = list(refs)

    def take(n):
        out = refs[:n]
        del refs[:n]
        return out

    mixer_in = take(15)
    output_ref, residual_ref, norm_gain_ref = take(3)
    shards = take(3)
    (out_ref,) = take(1)
    (normed,) = take(1)
    mixer_scratch = take(counts[0])
    weight, residual, x, after, load_sem = take(5)
    project_scratch = take(12)
    feed_scratch = take(11)
    (weights,) = take(1)
    sems = take(8)
    service = Gatherer(peers, shards, weights, sems)
    service.begin()
    loads = (
        pltpu.make_async_copy(output_ref, weight, load_sem.at[0]),
        pltpu.make_async_copy(residual_ref, residual, load_sem.at[1]),
    )
    for load in loads:
        load.start()
    at = mixer_part(peers, service, *mixer_in, normed, *mixer_scratch)
    for load in loads:
        load.wait()
    project_part(
        service, at, normed, weight, residual, norm_gain_ref, x, after, *project_scratch
    )
    feed_part(x, weights, after, out_ref, *feed_scratch)
    service.drain()


def layer(arrays, output_matrix, residual, norm_gain, shards, peers):
    length = arrays[0].shape[0]
    channels = arrays[0].shape[1]
    rows, width = residual.shape
    span = sum(a.shape[1] for a in arrays[:5])
    depth, units = shards[0].shape
    count = length // CH
    hbm = pl.BlockSpec(memory_space=pltpu.HBM)
    vmem = pl.BlockSpec(memory_space=pltpu.VMEM)
    dma = pltpu.SemaphoreType.DMA
    chips = peers // 2
    mixer_scratch = [
        pltpu.VMEM((PAD + length, span), BF16),
        pltpu.VMEM((length, channels), BF16),
        pltpu.VMEM((length, 384), BF16),
        pltpu.VMEM((length, 512), BF16),
        pltpu.VMEM((length, channels), BF16),
        pltpu.VMEM((length, 16), F32),
        pltpu.VMEM((count, 16, CH), F32),
        pltpu.VMEM((count, 1, 16), F32),
        pltpu.VMEM((count, 384, 256), F32),
        pltpu.VMEM((count, 384, 256), BF16),
        pltpu.VMEM((length, channels), F32),
        pltpu.VMEM((384, 256), F32),
        pltpu.VMEM((384, 256), BF16),
        pltpu.VMEM((400, 256), BF16),
        pltpu.VMEM((400, 256), BF16),
        pltpu.VMEM((384, 256), BF16),
        pltpu.VMEM((384, 256), BF16),
        dma((6,)),
        dma((5,)),
        dma((5,)),
        dma((2,)),
        dma((2,)),
        dma((384 // PIECE,)),
        dma((384 // PIECE,)),
    ]
    scratch = (
        [pltpu.VMEM((length, channels), BF16)]
        + mixer_scratch
        + [
            pltpu.VMEM(output_matrix.shape, BF16),
            pltpu.VMEM((rows, width), BF16),
            pltpu.VMEM((4 * rows, width), BF16),
            pltpu.VMEM((rows, width), BF16),
            dma((2,)),
        ]
        + reducer_scratch(rows, width)
        + [dma((ROW_PARTS, 6)), dma((ROW_PARTS, 6))]
        + reducer_scratch(rows, width)
        + [pltpu.VMEM((rows, units), BF16)]
        + [pltpu.VMEM((peers * depth, 3 * units), BF16)]
        + [
            dma((3,)),
            dma((PARTS * chips,)),
            dma((PARTS * chips,)),
            dma((PARTS * chips,)),
            dma((PARTS * chips,)),
            dma((PARTS * chips,)),
            dma((PARTS * chips,)),
            pltpu.SemaphoreType.REGULAR,
        ]
    )
    return pl.pallas_call(
        functools.partial(layer_kernel, peers, (len(mixer_scratch),)),
        out_shape=jax.ShapeDtypeStruct((rows, width), BF16),
        in_specs=[hbm] * 6 + [vmem] * 9 + [hbm, hbm, vmem] + [hbm] * 3,
        out_specs=vmem,
        scratch_shapes=scratch,
        compiler_params=pltpu.CompilerParams(
            collective_id=1, has_side_effects=True, vmem_limit_bytes=62 * 1024 * 1024
        ),
        cost_estimate=pl.CostEstimate(
            flops=40_000_000_000, bytes_accessed=20_000_000, transcendentals=0
        ),
        name="layer",
    )(*arrays, output_matrix, residual, norm_gain, *shards)


def on_device(
    residual,
    value_projected,
    gate_projected,
    wide_key_rows,
    wide_query_rows,
    narrow_key_rows,
    narrow_query_rows,
    step_before_softplus,
    extra_log_decay,
    log_decay_rate,
    value_kernel,
    wide_key_kernel,
    wide_query_kernel,
    narrow_key_kernel,
    narrow_query_kernel,
    head_norm_gain,
    output_matrix,
    feedforward_norm_gain,
    gate_matrix,
    up_matrix,
    down_matrix,
):
    return layer(
        [
            value_projected,
            wide_key_rows,
            wide_query_rows,
            narrow_key_rows,
            narrow_query_rows,
            gate_projected,
            step_before_softplus.T,
            extra_log_decay.T,
            log_decay_rate[None],
            value_kernel,
            wide_key_kernel,
            wide_query_kernel,
            narrow_key_kernel,
            narrow_query_kernel,
            head_norm_gain[None],
        ],
        output_matrix,
        residual,
        feedforward_norm_gain[None],
        (gate_matrix, up_matrix, down_matrix),
        lax.axis_size("sp"),
    )


def solution(mesh):
    in_specs = (
        P(("grp", "sp", "tp"), None),
        P(("grp", "sp"), "tp"),
        P(("grp", "sp"), "tp"),
        P(("grp", "sp"), "tp"),
        P(("grp", "sp"), "tp"),
        P(("grp", "sp"), "tp"),
        P(("grp", "sp"), "tp"),
        P(("grp", "sp"), "tp"),
        P(("grp", "sp"), "tp"),
        P("tp"),
        P(None, "tp"),
        P(None, "tp"),
        P(None, "tp"),
        P(None, "tp"),
        P(None, "tp"),
        P("tp"),
        P("tp", None),
        P(),
        P("sp", "tp"),
        P("sp", "tp"),
        P("sp", "tp"),
    )
    out_specs = P(("grp", "sp", "tp"), None)
    return jax.shard_map(
        on_device, mesh=mesh, in_specs=in_specs, out_specs=out_specs, check_vma=False
    )
```

```python
import functools
import jax
import jax.numpy as jnp
from jax import lax
from jax.experimental import pallas as pl
from jax.experimental.pallas import tpu as pltpu
from jax.sharding import PartitionSpec as P

F32 = jnp.float32
BF16 = jnp.bfloat16
MESH = pl.DeviceIdType.MESH
CH = 128
PAD = 16
PIECE = 16
GROUP_Q = (0, 256, 128, 384)
GROUP_K = (0, 256, 128, 256)
ROW_GROUP = ((0, 128, 0), (128, 256, 2), (256, 320, 1), (320, 384, 3))
HIGH = lax.Precision.HIGHEST


def pair_lanes(columns, head):
    rows = columns.shape[0]
    lane = lax.broadcasted_iota(jnp.int32, (rows, 128), 1)
    return jnp.where(
        lane < 64,
        jnp.broadcast_to(columns[:, head : head + 1], (rows, 128)),
        jnp.broadcast_to(columns[:, head + 1 : head + 2], (rows, 128)),
    )


def quad_lanes(columns, group):
    return jnp.concatenate(
        [pair_lanes(columns, 4 * group), pair_lanes(columns, 4 * group + 2)], axis=1
    )


def silu(x):
    return x / (1.0 + jnp.exp(-x))


def matmul(a, b, dims=((1,), (0,)), precision=None):
    return lax.dot_general(a, b, (dims, ((), ())), preferred_element_type=F32, precision=precision)


def group_of_row(row):
    for low, high, group in ROW_GROUP:
        if low <= row < high:
            return group


def mixer_part(
    peers,
    service,
    value_ref,
    wk_ref,
    wq_ref,
    nk_ref,
    nq_ref,
    gate_ref,
    step_ref,
    extra_ref,
    rate_ref,
    vker_ref,
    wkker_ref,
    wqker_ref,
    nkker_ref,
    nqker_ref,
    gain_ref,
    normed_ref,
    xpad,
    ubuf,
    kbuf,
    qbuf,
    gbuf,
    rcol,
    qrow,
    total,
    ebuf,
    hbuf,
    ybuf,
    hent,
    entered_ref,
    half_out,
    half_in,
    chain_in,
    chain_out,
    pair_out,
    pair_in,
    give,
    local_sem,
    rim_send,
    rim_recv,
    swap_send,
    swap_recv,
    chain_send,
    chain_recv,
):
    length = value_ref.shape[0]
    count = length // CH
    me = lax.axis_index("sp")
    inputs = (value_ref, wk_ref, wq_ref, nk_ref, nq_ref)
    spans = []
    at = 0
    for ref in inputs:
        spans.append((at, at + ref.shape[1]))
        at += ref.shape[1]
    loads = [
        pltpu.make_async_copy(
            ref, xpad.at[pl.ds(PAD, length), pl.ds(low, high - low)], local_sem.at[n]
        )
        for n, (ref, (low, high)) in enumerate(zip(inputs, spans))
    ]
    loads.append(pltpu.make_async_copy(gate_ref, gbuf, local_sem.at[len(inputs)]))
    for load in loads:
        load.start()
    core = lax.rem(me, 2)
    chip = me // 2
    chips = peers // 2
    partner = me + 1 - 2 * core

    def send_to(peer, source, target, send, recv):
        return pltpu.make_async_remote_copy(
            src_ref=source,
            dst_ref=target,
            send_sem=send,
            recv_sem=recv,
            device_id={"sp": peer},
            device_id_type=MESH,
        )

    def rim(n):
        low, high = spans[n]
        return send_to(
            lax.rem(me + 1, peers),
            inputs[n].at[pl.ds(length - PAD, PAD)],
            xpad.at[pl.ds(0, PAD), pl.ds(low, high - low)],
            rim_send.at[n],
            rim_recv.at[n],
        )

    greet_all(me, peers, service.reply)
    service.open()

    @pl.when(me < peers - 1)
    def _():
        for n in range(len(inputs)):
            rim(n).start()

    for load in loads[:-1]:
        load.wait()

    row_id = lax.broadcasted_iota(jnp.int32, (CH, CH), 0)
    col_id = lax.broadcasted_iota(jnp.int32, (CH, CH), 1)
    lower = row_id >= col_id
    tril = lower.astype(F32)
    triu = (row_id <= col_id).astype(F32)
    eye = (row_id == col_id).astype(F32)
    left = lax.broadcasted_iota(jnp.int32, (CH, 128), 1) < 64
    diagonal = lax.broadcasted_iota(jnp.int32, (16, 16), 0) == lax.broadcasted_iota(
        jnp.int32, (16, 16), 1
    )
    rate = -jnp.sum(
        jnp.where(diagonal, jnp.broadcast_to(jnp.exp(rate_ref[...]), (16, 16)), 0.0),
        axis=1,
        keepdims=True,
    )
    kernels = (vker_ref, wkker_ref, wqker_ref, nkker_ref, nqker_ref)

    def conv_tile(base, which, tile):
        low = spans[which][0] + 128 * tile
        columns = pl.ds(low, 128)
        before = xpad[pl.ds(base, PAD), columns].astype(F32)[PAD - 8 :]
        here = xpad[pl.ds(base + PAD, CH), columns].astype(F32)
        rows = jnp.concatenate([before, here], axis=0)
        taps = kernels[which][:, 128 * tile : 128 * tile + 128].astype(F32)
        acc = here * taps[3:4]
        for tap in range(3):
            acc = acc + pltpu.roll(rows, 3 - tap, 0)[8:] * taps[tap : tap + 1]
        return silu(acc)

    def first_pass(i, carry):
        c = lax.rem(i + 1, count)
        base = pl.multiple_of(c * CH, CH)

        @pl.when(i == count - 1)
        def _():
            @pl.when(me > 0)
            def _():
                for n in range(len(inputs)):
                    rim(n).wait_recv()

            @pl.when(me == 0)
            def _():
                xpad[0:PAD, :] = jnp.zeros((PAD, xpad.shape[1]), BF16)

        here = pl.ds(base, CH)
        dt_row = step_ref[:, here]
        dt_row = jnp.maximum(dt_row, 0.0) + jnp.log(1.0 + jnp.exp(-jnp.abs(dt_row)))
        a = rate * dt_row + extra_ref[:, here]
        r = matmul(tril, a, ((1,), (1,)), HIGH)
        r_row = matmul(a, triu, precision=HIGH)
        dt = matmul(eye, dt_row, ((1,), (1,)), HIGH)
        rcol[here, :] = r
        qrow[c] = r_row - jnp.log(dt_row)
        end = r[CH - 1 : CH, :]
        total[c] = end
        fade = dt * jnp.exp(end - r)
        for tile in range(2):
            kbuf[here, 128 * tile : 128 * tile + 128] = conv_tile(base, 1, tile).astype(BF16)
            qbuf[here, 128 * tile : 128 * tile + 128] = conv_tile(base, 2, tile).astype(BF16)
        kbuf[here, 256:384] = conv_tile(base, 3, 0).astype(BF16)
        narrow_q = conv_tile(base, 4, 0)
        qbuf[here, 256:384] = jnp.where(left, narrow_q, 0.0).astype(BF16)
        qbuf[here, 384:512] = jnp.where(left, 0.0, narrow_q).astype(BF16)
        for group in range(4):
            parts = []
            for half in range(2):
                pair = 2 * group + half
                u = conv_tile(base, 0, pair).astype(BF16)
                ubuf[here, 128 * pair : 128 * pair + 128] = u
                parts.append((u.astype(F32) * pair_lanes(fade, 2 * pair)).astype(BF16))
            v = jnp.concatenate(parts, axis=1)
            k = kbuf[here, GROUP_K[group] : GROUP_K[group] + 128]
            e = matmul(k, v, ((0,), (0,)))
            if group == 0:
                ebuf[c, 0:128, :] = e
            elif group == 2:
                ebuf[c, 128:256, :] = e
            elif group == 1:
                ebuf[c, 256:320, :] = e[0:64]
            else:
                ebuf[c, 320:384, :] = e[64:128]
        service.run(20 + 14 * i, 34 + 14 * i)
        return carry

    lax.fori_loop(0, count, first_pass, 0)

    offsets = [jnp.zeros((1, 16), F32)]
    for c in range(count):
        offsets.append(offsets[-1] + total[c])
    whole = offsets[-1]
    for low, high, group in ROW_GROUP:
        state = jnp.zeros((high - low, 256), F32)
        for c in range(count):
            hbuf[c, low:high, :] = state.astype(BF16)
            state = state * jnp.exp(quad_lanes(total[c], group)) + ebuf[c, low:high, :]
        hent[low:high, :] = state

    log_total = [quad_lanes(whole, group) for group in range(4)]
    sub = lax.broadcasted_iota(jnp.int32, (16, 256), 0)
    swap = send_to(partner, half_out, half_in, swap_send.at[0], swap_recv.at[0])

    @pl.when(core == 0)
    def _():
        half_out[0:384, :] = hent[...].astype(BF16)
        lines = jnp.zeros((16, 256), F32)
        for group in range(4):
            lines = jnp.where(
                sub == group, jnp.broadcast_to(log_total[group], (16, 256)), lines
            )
        half_out[384:400, :] = lines.astype(BF16)
        swap.start()

    def second_pass(c, start):
        here = pl.ds(pl.multiple_of(c * CH, CH), CH)
        r = rcol[here, :]
        fade_out = jnp.exp(r)
        for group in range(4):
            q = qbuf[here, GROUP_Q[group] : GROUP_Q[group] + 128]
            k = kbuf[here, GROUP_K[group] : GROUP_K[group] + 128]
            score = matmul(q, k, ((1,), (1,)))
            row = 0 if group == 0 else 128 if group == 2 else 256
            outer = matmul(q, hbuf[c, row : row + 128, :])
            for half in range(2):
                pair = 2 * group + half
                weights = []
                for head in (2 * pair, 2 * pair + 1):
                    gap = jnp.broadcast_to(r[:, head : head + 1], (CH, CH)) - qrow[c, head : head + 1, :]
                    w = score * jnp.exp(jnp.where(lower, gap, -jnp.inf))
                    weights.append(w.astype(BF16))
                u = ubuf[here, 128 * pair : 128 * pair + 128].astype(F32)
                both = jnp.concatenate(
                    [jnp.where(left, u, 0.0).astype(BF16), jnp.where(left, 0.0, u).astype(BF16)],
                    axis=0,
                )
                inner = matmul(jnp.concatenate(weights, axis=1), both)
                ybuf[here, 128 * pair : 128 * pair + 128] = (
                    inner + outer[:, 128 * half : 128 * half + 128] * pair_lanes(fade_out, 2 * pair)
                )
        service.run(start + 11 * c, start + 11 * c + 11)
        return start

    early = jnp.where(chip == 0, 1, count)
    service.run(20 + 14 * count, 120)
    lax.fori_loop(0, early, second_pass, 120)
    odd = lax.rem(chip, 2)
    sends_on = (chip < chips - 1) & (core * odd == 1)

    def link(piece, hops):
        rows = pl.ds(piece * PIECE, PIECE)
        return send_to(
            lax.rem(me + 2 * hops, peers),
            chain_out.at[rows],
            chain_in.at[rows],
            chain_send.at[hops - 1, piece],
            chain_recv.at[piece],
        )

    hand = send_to(partner, give, entered_ref, swap_send.at[1], swap_recv.at[1])
    couple = send_to(
        lax.rem(me + 2, peers), pair_out, pair_in, swap_send.at[2], swap_recv.at[2]
    )

    @pl.when(core == 1)
    def _():
        swap.wait_recv()
        lines = half_in[384:400, :].astype(F32)
        fade_0 = [jnp.exp(lines[group : group + 1]) for group in range(4)]
        fade_1 = [jnp.exp(line) for line in log_total]

        @pl.when(odd == 0)
        def _():
            for at in range(0, 384, 16):
                rows = slice(at, at + 16)
                pair_out[rows, :] = (
                    half_in[rows, :].astype(F32) * fade_1[group_of_row(at)] + hent[rows, :]
                ).astype(BF16)
            both = jnp.zeros((16, 256), F32)
            for group in range(4):
                line = lines[group : group + 1] + log_total[group]
                both = jnp.where(sub == group, jnp.broadcast_to(line, (16, 256)), both)
            pair_out[384:400, :] = both.astype(BF16)
            couple.start()

        @pl.when(odd == 1)
        def _():
            couple.wait_recv()

        @pl.when(odd == 0)
        def _():
            pair_in[...] = jnp.zeros_like(pair_in)

        @pl.when(chip < 2)
        def _():
            chain_in[...] = jnp.zeros_like(chain_in)

        pair_lines = pair_in[384:400, :].astype(F32)
        fade_pair = [jnp.exp(pair_lines[group : group + 1]) for group in range(4)]

        for piece in range(384 // PIECE):

            @pl.when(chip > 1)
            def _():
                link(piece, 1).wait_recv()

            for at in range(piece * PIECE, piece * PIECE + PIECE, 16):
                group = group_of_row(at)
                rows = slice(at, at + 16)
                prior = (
                    chain_in[rows, :].astype(F32) * fade_pair[group]
                    + pair_in[rows, :].astype(F32)
                )
                second = prior * fade_0[group] + half_in[rows, :].astype(F32)
                chain_out[rows, :] = (second * fade_1[group] + hent[rows, :]).astype(BF16)
                entered_ref[rows, :] = second.astype(BF16)
                give[rows, :] = prior.astype(BF16)

            @pl.when(sends_on)
            def _():
                link(piece, 2).start()
                link(piece, 1).start()

        hand.start()

    service.run(120 + 11 * early, 130 + 11 * early)
    lax.fori_loop(early, count, second_pass, 130)
    at = 130 + 11 * count
    loads[-1].wait()

    @pl.when(core == 0)
    def _():
        swap.wait_send()
        hand.wait_recv()

    @pl.when(core == 1)
    def _():
        hand.wait_send()

        @pl.when(odd == 0)
        def _():
            couple.wait_send()

    @pl.when(sends_on)
    def _():
        for piece in range(384 // PIECE):
            link(piece, 1).wait_send()
            link(piece, 2).wait_send()

    @pl.when(me < peers - 1)
    def _():
        for n in range(len(inputs)):
            rim(n).wait_send()

    ones = (
        (row_id < 64) == (col_id < 64)
    ).astype(BF16)

    for c in range(count):
        here = slice(c * CH, c * CH + CH)
        reach = jnp.exp(rcol[here, :] + offsets[c])
        for group in range(4):
            q = qbuf[here, GROUP_Q[group] : GROUP_Q[group] + 128]
            row = 0 if group == 0 else 128 if group == 2 else 256
            entered = matmul(q, entered_ref[row : row + 128, :])
            for half in range(2):
                pair = 2 * group + half
                lanes = slice(128 * pair, 128 * pair + 128)
                y = ybuf[here, lanes]
                y = y + entered[:, 128 * half : 128 * half + 128] * pair_lanes(reach, 2 * pair)
                gated = y * silu(gbuf[here, lanes].astype(F32))
                square = matmul((gated * gated).astype(BF16), ones)
                scale = lax.rsqrt(square * (1.0 / 64.0) + 1e-06)
                normed_ref[here, lanes] = (
                    gated * scale * gain_ref[pair : pair + 1, :].astype(F32)
                ).astype(BF16)
        service.run(at, at + 6)
        at = at + 6
    return at


ROW_PARTS = 2


def silu_gate(x):
    return x / (1.0 + jnp.exp(-x))


class Reducer:
    def __init__(self, axis, buffers, send, recv):
        self.me = lax.axis_index(axis)
        self.right = lax.rem(self.me + 1, 4)
        self.left = lax.rem(self.me + 3, 4)
        self.far = lax.rem(self.me + 2, 4)
        self.axis = axis
        (self.blocks, self.own, self.relay_r, self.relay_l, self.comb_r, self.comb_l,
         self.from_l, self.from_r) = buffers
        self.send, self.recv = send, recv
        self.rows = self.own.shape[0] // ROW_PARTS
        self.half = self.own.shape[1] // 2

    def copy(self, part, index, source, target, to):
        return pltpu.make_async_remote_copy(
            src_ref=source,
            dst_ref=target,
            send_sem=self.send.at[part, index],
            recv_sem=self.recv.at[part, index],
            device_id={self.axis: to},
            device_id_type=MESH,
        )

    def leg(self, part, index):
        rows = pl.ds(part * self.rows, self.rows)
        a, b = pl.ds(0, self.half), pl.ds(self.half, self.half)
        source, target = (
            (self.blocks.at[0, rows, a], self.relay_r.at[rows]),
            (self.blocks.at[1, rows, b], self.from_l.at[rows, b]),
            (self.comb_r.at[rows], self.from_l.at[rows, a]),
            (self.blocks.at[0, rows, b], self.relay_l.at[rows]),
            (self.blocks.at[2, rows, a], self.from_r.at[rows, a]),
            (self.comb_l.at[rows], self.from_r.at[rows, b]),
        )[index]
        return self.copy(part, index, source, target, self.right if index < 3 else self.left)

    def combine(self, part):
        step = 32

        for n, block, low, relay, comb in (
            (0, 1, 0, self.relay_r, self.comb_r),
            (3, 2, self.half, self.relay_l, self.comb_l),
        ):
            self.leg(part, n).wait_recv()

            def body(i, carry, block=block, low=low, relay=relay, comb=comb):
                rows = pl.ds(pl.multiple_of(part * self.rows + i * step, 16), step)
                comb[rows, :] = (
                    self.blocks[block, rows, low : low + self.half].astype(F32)
                    + relay[rows, :].astype(F32)
                ).astype(BF16)
                return carry

            lax.fori_loop(0, self.rows // step, body, 0)
            self.leg(part, n + 2).start()

    def wait_final(self, part):
        for n in (1, 2, 4, 5):
            self.leg(part, n).wait_recv()

    def wait_sends(self):
        for part in range(ROW_PARTS):
            for n in range(6):
                self.leg(part, n).wait_send()

    def total(self, rows):
        return (
            self.own[rows, :]
            + self.from_l[rows, :].astype(F32)
            + self.from_r[rows, :].astype(F32)
        )


def reducer_scratch(rows, width):
    half = width // 2
    dma = pltpu.SemaphoreType.DMA
    return [
        pltpu.VMEM((3, rows, width), BF16),
        pltpu.VMEM((rows, width), F32),
        pltpu.VMEM((rows, half), BF16),
        pltpu.VMEM((rows, half), BF16),
        pltpu.VMEM((rows, half), BF16),
        pltpu.VMEM((rows, half), BF16),
        pltpu.VMEM((rows, width), BF16),
        pltpu.VMEM((rows, width), BF16),
        dma((ROW_PARTS, 6)),
        dma((ROW_PARTS, 6)),
    ]


def project_part(
    service, at, normed_ref, weight_ref, residual_ref, gain_ref, x_ref, after_ref, *scratch
):
    buffers, (send, recv, gsend, grecv) = scratch[:8], scratch[8:]
    red = Reducer("tp", buffers, send, recv)
    blocks, own = buffers[0], buffers[1]
    rows, width = own.shape
    half = width // 2

    def make(owner, slot):
        source = pl.ds(pl.multiple_of(owner * rows, 64), rows)

        def body(j, carry):
            columns = pl.ds(pl.multiple_of(j * 256, 256), 256)
            product = matmul(normed_ref[source, :], weight_ref[:, columns])
            if slot is None:
                own[:, columns] = product
            else:
                blocks[slot, :, columns] = product.astype(BF16)
            return carry

        lax.fori_loop(0, width // 256, body, 0)

    make(red.far, 0)
    red.leg(0, 0).start()
    red.leg(0, 3).start()
    service.run(at, at + 14)
    make(red.right, 1)
    red.leg(0, 1).start()
    service.run(at + 14, at + 28)
    make(red.left, 2)
    red.leg(0, 4).start()
    service.run(at + 28, at + 42)
    make(red.me, None)
    service.open_last()
    service.run(at + 42, at + 65)

    part_rows = red.rows

    def spread(part, index, owner, low, to):
        where = x_ref.at[
            pl.ds(pl.multiple_of(owner * rows + part * part_rows, 32), part_rows),
            pl.ds(low, half),
        ]
        return pltpu.make_async_remote_copy(
            src_ref=where,
            dst_ref=where,
            send_sem=gsend.at[part, index],
            recv_sem=grecv.at[part, index],
            device_id={"tp": to},
            device_id_type=MESH,
        )

    def leaving(part, index):
        owner = (red.me, red.me, red.left, red.me, red.me, red.right)[index]
        low = (0, half, 0, half, 0, half)[index]
        return spread(part, index, owner, low, red.right if index < 3 else red.left)

    def coming(part, index):
        owner = (red.left, red.left, red.far, red.right, red.right, red.far)[index]
        low = (0, half, 0, half, 0, half)[index]
        return spread(part, index, owner, low, red.right if index < 3 else red.left)

    gain = gain_ref[...].astype(F32)
    gain = jnp.concatenate([gain[n : n + 1] for n in range(width // 128)], axis=1)

    def finish(part):
        red.wait_final(part)

        def body(i, carry):
            at = part * part_rows + i * 16
            here = pl.ds(pl.multiple_of(at, 16), 16)
            after = (residual_ref[here, :].astype(F32) + red.total(here)).astype(BF16)
            after_ref[here, :] = after
            x = after.astype(F32)
            scale = lax.rsqrt(jnp.mean(x * x, axis=1, keepdims=True) + 1e-06)
            x_ref[pl.ds(pl.multiple_of(red.me * rows + at, 16), 16), :] = (
                x * scale * gain
            ).astype(BF16)
            return carry

        lax.fori_loop(0, part_rows // 16, body, 0)
        for n in (0, 3, 1, 4):
            leaving(part, n).start()

    def pass_on(part):
        for n in (0, 3):
            coming(part, n).wait_recv()
            leaving(part, n + 2).start()

    red.combine(0)
    for n in (0, 3, 1, 4):
        red.leg(1, n).start()
    service.run(at + 65, at + 110)
    finish(0)
    service.run(at + 110, at + 170)
    red.combine(1)
    service.run(at + 170, at + 270)
    pass_on(0)
    service.run(at + 270, at + 320)
    finish(1)
    service.run(at + 320, at + 430)
    pass_on(1)
    service.close(at + 430)
    for part in range(ROW_PARTS):
        for n in (1, 2, 4, 5):
            coming(part, n).wait_recv()
        for n in range(6):
            leaving(part, n).wait_send()
    red.wait_sends()


def feed_part(x_ref, weight_ref, after_ref, out_ref, *scratch):
    buffers, (send, recv, hidden) = scratch[:8], scratch[8:]
    red = Reducer("tp", buffers, send, recv)
    blocks, own = buffers[0], buffers[1]
    rows, width = own.shape
    units = weight_ref.shape[1] // 3
    tiles = units // 256

    def make(owner, slot):
        source = pl.ds(pl.multiple_of(owner * rows, 64), rows)

        def inner(j, carry):
            low = pl.multiple_of(j * 256, 256)
            x = x_ref[source, :]
            gate = matmul(x, weight_ref[:, pl.ds(low, 256)])
            up = matmul(x, weight_ref[:, pl.ds(pl.multiple_of(units + low, 256), 256)])
            hidden[:, pl.ds(low, 256)] = (silu_gate(gate) * up).astype(BF16)
            return carry

        lax.fori_loop(0, tiles, inner, 0)

        def body(j, carry):
            columns = pl.ds(pl.multiple_of(j * 256, 256), 256)
            product = matmul(
                hidden[...], weight_ref[columns, 2 * units : 3 * units], ((1,), (1,))
            )
            if slot is None:
                own[:, columns] = product
            else:
                blocks[slot, :, columns] = product.astype(BF16)
            return carry

        lax.fori_loop(0, width // 256, body, 0)

    make(red.far, 0)
    red.leg(0, 0).start()
    red.leg(0, 3).start()
    make(red.right, 1)
    red.leg(0, 1).start()
    make(red.left, 2)
    red.leg(0, 4).start()
    red.combine(0)
    for n in (0, 3, 1, 4):
        red.leg(1, n).start()
    make(red.me, None)

    def finish(part):
        red.wait_final(part)

        def body(i, carry):
            here = pl.ds(pl.multiple_of(part * red.rows + i * 16, 16), 16)
            out_ref[here, :] = (
                after_ref[here, :].astype(F32) + 0.5 * red.total(here)
            ).astype(BF16)
            return carry

        lax.fori_loop(0, red.rows // 16, body, 0)

    finish(0)
    red.combine(1)
    finish(1)
    red.wait_sends()


def greet_all(me, peers, reply):
    core = lax.rem(me, 2)
    chip = me // 2
    last = peers // 2 - 1
    side = lax.axis_index("tp")
    barrier = pltpu.get_barrier_semaphore()

    def hail(axis, other):
        pl.semaphore_signal(barrier, inc=1, device_id={axis: other}, device_id_type=MESH)

    hail("tp", lax.rem(side + 1, 4))
    hail("tp", lax.rem(side + 3, 4))
    hail("sp", me + 1 - 2 * core)

    @pl.when(chip > 0)
    def _():
        hail("sp", me - 1 - core)
        hail("sp", me - 2)

    @pl.when(chip < last)
    def _():
        hail("sp", me + 2)

    below = (chip > 0).astype(jnp.int32)
    above = (chip < last).astype(jnp.int32)
    odd = lax.rem(chip, 2)

    @pl.when((chip > 1) & (core * odd == 1))
    def _():
        hail("sp", me - 4)

    far = above * core * odd
    pl.semaphore_wait(barrier, 3 + below + above + 2 * above * core + 1 - above + far)

    @pl.when(chip == 0)
    def _():
        hail("sp", me + 2 * last)

    @pl.when(chip == last)
    def _():
        pl.semaphore_signal(
            reply, inc=1, device_id={"sp": me - 2 * last}, device_id_type=MESH
        )


PARTS = 3


class Gatherer:
    def __init__(self, peers, shards, weights, sems):
        self.me = lax.axis_index("sp")
        self.peers = peers
        self.core = lax.rem(self.me, 2)
        self.chip = self.me // 2
        self.chips = peers // 2
        self.up_steps = PARTS * (self.chips // 2 - 1)
        self.down_steps = PARTS * (self.chips - 1) - self.up_steps
        self.shards, self.weights = shards, weights
        (self.own_sem, self.up_send, self.up_recv, self.down_send, self.down_recv,
         self.side_send, self.side_recv, self.reply) = sems
        self.depth = shards[0].shape[0]

    def own(self, n):
        return pltpu.make_async_copy(
            self.shards[n], self.place(self.chip, self.core, n), self.own_sem.at[n]
        )

    def place(self, chip, core, part):
        units = self.shards[0].shape[1]
        return self.weights.at[
            pl.ds(pl.multiple_of((2 * chip + core) * self.depth, 64), self.depth),
            pl.ds(pl.multiple_of(part * units, 128), units),
        ]

    def begin(self):
        for n in range(3):
            self.own(n).start()

    def move(self, place, to, send, recv):
        return pltpu.make_async_remote_copy(
            src_ref=place,
            dst_ref=place,
            send_sem=send,
            recv_sem=recv,
            device_id={"sp": to},
            device_id_type=MESH,
        )

    def up(self, k, hops=0):
        distance = k // PARTS + hops
        origin = lax.rem(self.chip + self.chips - distance, self.chips)
        to = lax.rem(self.me + 2, self.peers)
        place = self.place(origin, self.core, lax.rem(k, PARTS))
        return self.move(place, to, self.up_send.at[k], self.up_recv.at[k])

    def down(self, k, hops=0):
        distance = k // PARTS + hops
        origin = lax.rem(self.chip + distance, self.chips)
        to = lax.rem(self.me + self.peers - 2, self.peers)
        place = self.place(origin, self.core, lax.rem(k, PARTS))
        return self.move(place, to, self.down_send.at[k], self.down_recv.at[k])

    def side(self, k, core):
        to = self.me + 1 - 2 * self.core
        place = self.place(k // PARTS, core, lax.rem(k, PARTS))
        return self.move(place, to, self.side_send.at[k], self.side_recv.at[k])

    def open(self):
        for n in range(PARTS):
            self.own(n).wait()
            self.up(n).start()

            @pl.when(self.chip > 0)
            def _():
                self.down(n).start()

            self.side(self.chip * PARTS + n, self.core).start()

    def open_last(self):
        @pl.when(self.chip == 0)
        def _():
            pl.semaphore_wait(self.reply, 1)
            for n in range(PARTS):
                self.down(n).start()

    def due(self, at):
        near = jnp.maximum((at - 55) // 20, 0)
        wrapped = (at - 279) // 20
        limit = PARTS * self.chip
        up = jnp.minimum(
            jnp.where(wrapped > limit, wrapped, jnp.minimum(near, limit)), self.up_steps
        )
        down = jnp.minimum(jnp.maximum((at - 90) // 27, 0), self.down_steps)
        down = jnp.where((self.chip == 0) & (at < 275), 0, down)
        return up, down

    def steps(self, first, then):
        def step_up(i, carry):
            self.up(i, 1).wait_recv()

            @pl.when(i + PARTS < self.up_steps)
            def _():
                self.up(i + PARTS).start()

            origin = lax.rem(self.chip + self.chips - i // PARTS - 1, self.chips)
            self.side(origin * PARTS + lax.rem(i, PARTS), self.core).start()
            return carry

        def step_down(i, carry):
            self.down(i, 1).wait_recv()

            @pl.when(i + PARTS < self.down_steps)
            def _():
                self.down(i + PARTS).start()

            origin = lax.rem(self.chip + i // PARTS + 1, self.chips)
            self.side(origin * PARTS + lax.rem(i, PARTS), self.core).start()
            return carry

        lax.fori_loop(first[0], then[0], step_up, 0)
        lax.fori_loop(first[1], then[1], step_down, 0)

    def run(self, at, until):
        self.steps(self.due(at), self.due(until))

    def close(self, at):
        self.steps(self.due(at), (self.up_steps, self.down_steps))

        def arrive(i, carry):
            self.side(i, 1 - self.core).wait_recv()
            return carry

        lax.fori_loop(0, PARTS * self.chips, arrive, 0)

    def drain(self):
        def up(i, carry):
            self.up(i).wait_send()
            return carry

        def down(i, carry):
            self.down(i).wait_send()
            return carry

        def side(i, carry):
            self.side(i, self.core).wait_send()
            return carry

        lax.fori_loop(0, self.up_steps, up, 0)
        lax.fori_loop(0, self.down_steps, down, 0)
        lax.fori_loop(0, PARTS * self.chips, side, 0)


def layer_kernel(peers, counts, *refs):
    refs = list(refs)

    def take(n):
        out = refs[:n]
        del refs[:n]
        return out

    mixer_in = take(15)
    output_ref, residual_ref, norm_gain_ref = take(3)
    shards = take(3)
    (out_ref,) = take(1)
    (normed,) = take(1)
    mixer_scratch = take(counts[0])
    weight, residual, x, after, load_sem = take(5)
    project_scratch = take(12)
    feed_scratch = take(11)
    (weights,) = take(1)
    sems = take(8)
    service = Gatherer(peers, shards, weights, sems)
    service.begin()
    loads = (
        pltpu.make_async_copy(output_ref, weight, load_sem.at[0]),
        pltpu.make_async_copy(residual_ref, residual, load_sem.at[1]),
    )
    for load in loads:
        load.start()
    at = mixer_part(peers, service, *mixer_in, normed, *mixer_scratch)
    for load in loads:
        load.wait()
    project_part(
        service, at, normed, weight, residual, norm_gain_ref, x, after, *project_scratch
    )
    feed_part(x, weights, after, out_ref, *feed_scratch)
    service.drain()


def layer(arrays, output_matrix, residual, norm_gain, shards, peers):
    length = arrays[0].shape[0]
    channels = arrays[0].shape[1]
    rows, width = residual.shape
    span = sum(a.shape[1] for a in arrays[:5])
    depth, units = shards[0].shape
    count = length // CH
    hbm = pl.BlockSpec(memory_space=pltpu.HBM)
    vmem = pl.BlockSpec(memory_space=pltpu.VMEM)
    dma = pltpu.SemaphoreType.DMA
    chips = peers // 2
    mixer_scratch = [
        pltpu.VMEM((PAD + length, span), BF16),
        pltpu.VMEM((length, channels), BF16),
        pltpu.VMEM((length, 384), BF16),
        pltpu.VMEM((length, 512), BF16),
        pltpu.VMEM((length, channels), BF16),
        pltpu.VMEM((length, 16), F32),
        pltpu.VMEM((count, 16, CH), F32),
        pltpu.VMEM((count, 1, 16), F32),
        pltpu.VMEM((count, 384, 256), F32),
        pltpu.VMEM((count, 384, 256), BF16),
        pltpu.VMEM((length, channels), F32),
        pltpu.VMEM((384, 256), F32),
        pltpu.VMEM((384, 256), BF16),
        pltpu.VMEM((400, 256), BF16),
        pltpu.VMEM((400, 256), BF16),
        pltpu.VMEM((384, 256), BF16),
        pltpu.VMEM((384, 256), BF16),
        pltpu.VMEM((400, 256), BF16),
        pltpu.VMEM((400, 256), BF16),
        pltpu.VMEM((384, 256), BF16),
        dma((6,)),
        dma((5,)),
        dma((5,)),
        dma((3,)),
        dma((3,)),
        dma((2, 384 // PIECE)),
        dma((384 // PIECE,)),
    ]
    scratch = (
        [pltpu.VMEM((length, channels), BF16)]
        + mixer_scratch
        + [
            pltpu.VMEM(output_matrix.shape, BF16),
            pltpu.VMEM((rows, width), BF16),
            pltpu.VMEM((4 * rows, width), BF16),
            pltpu.VMEM((rows, width), BF16),
            dma((2,)),
        ]
        + reducer_scratch(rows, width)
        + [dma((ROW_PARTS, 6)), dma((ROW_PARTS, 6))]
        + reducer_scratch(rows, width)
        + [pltpu.VMEM((rows, units), BF16)]
        + [pltpu.VMEM((peers * depth, 3 * units), BF16)]
        + [
            dma((3,)),
            dma((PARTS * chips,)),
            dma((PARTS * chips,)),
            dma((PARTS * chips,)),
            dma((PARTS * chips,)),
            dma((PARTS * chips,)),
            dma((PARTS * chips,)),
            pltpu.SemaphoreType.REGULAR,
        ]
    )
    return pl.pallas_call(
        functools.partial(layer_kernel, peers, (len(mixer_scratch),)),
        out_shape=jax.ShapeDtypeStruct((rows, width), BF16),
        in_specs=[hbm] * 6 + [vmem] * 9 + [hbm, hbm, vmem] + [hbm] * 3,
        out_specs=vmem,
        scratch_shapes=scratch,
        compiler_params=pltpu.CompilerParams(
            collective_id=1, has_side_effects=True, vmem_limit_bytes=62 * 1024 * 1024
        ),
        cost_estimate=pl.CostEstimate(
            flops=40_000_000_000, bytes_accessed=20_000_000, transcendentals=0
        ),
        name="layer",
    )(*arrays, output_matrix, residual, norm_gain, *shards)


def on_device(
    residual,
    value_projected,
    gate_projected,
    wide_key_rows,
    wide_query_rows,
    narrow_key_rows,
    narrow_query_rows,
    step_before_softplus,
    extra_log_decay,
    log_decay_rate,
    value_kernel,
    wide_key_kernel,
    wide_query_kernel,
    narrow_key_kernel,
    narrow_query_kernel,
    head_norm_gain,
    output_matrix,
    feedforward_norm_gain,
    gate_matrix,
    up_matrix,
    down_matrix,
):
    return layer(
        [
            value_projected,
            wide_key_rows,
            wide_query_rows,
            narrow_key_rows,
            narrow_query_rows,
            gate_projected,
            step_before_softplus.T,
            extra_log_decay.T,
            log_decay_rate[None],
            value_kernel,
            wide_key_kernel,
            wide_query_kernel,
            narrow_key_kernel,
            narrow_query_kernel,
            head_norm_gain.reshape(-1, 128),
        ],
        output_matrix,
        residual,
        feedforward_norm_gain.reshape(-1, 128),
        (gate_matrix, up_matrix, down_matrix),
        lax.axis_size("sp"),
    )


def solution(mesh):
    in_specs = (
        P(("grp", "sp", "tp"), None),
        P(("grp", "sp"), "tp"),
        P(("grp", "sp"), "tp"),
        P(("grp", "sp"), "tp"),
        P(("grp", "sp"), "tp"),
        P(("grp", "sp"), "tp"),
        P(("grp", "sp"), "tp"),
        P(("grp", "sp"), "tp"),
        P(("grp", "sp"), "tp"),
        P("tp"),
        P(None, "tp"),
        P(None, "tp"),
        P(None, "tp"),
        P(None, "tp"),
        P(None, "tp"),
        P("tp"),
        P("tp", None),
        P(),
        P("sp", "tp"),
        P("sp", "tp"),
        P("sp", "tp"),
    )
    out_specs = P(("grp", "sp", "tp"), None)
    return jax.shard_map(
        on_device, mesh=mesh, in_specs=in_specs, out_specs=out_specs, check_vma=False
    )
```
